32 devices in a mesh: grp: 2 (over y), sp: 8 (over z, core), tp: 2 (over x).
Axes of the slice: x: 2, y: 2, z: 4, core: 2. Of those that a mesh axis runs over, the one named last changes fastest.
Arguments:
- out_gate: bfloat16 [6144, 1024], P(('grp', 'sp'), 'tp'), parts along dimension 0, may hold values from -6 to 6
- in_gate: bfloat16 [6144, 1024], P(('grp', 'sp'), 'tp'), parts along dimension 0, may hold values from -6 to 6
- conv_input: bfloat16 [6144, 1024], P(('grp', 'sp'), 'tp'), parts along dimension 0, may hold values from -6 to 6
- doc_ids: int32 [6144], P(('grp', 'sp')), parts along dimension 0, may hold values from 0 to 3, never falling along the last dimension, each value on 1 to 1536 neighbouring positions
- residual: bfloat16 [6144, 2048], P(('grp', 'sp'), 'tp'), parts along dimension 0, may hold values from -6 to 6
- conv_taps: float32 [3, 1024], P(None, 'tp'), may hold values from -6 to 6
- mix_gain: float32 [1024], P('tp'), may hold values from 0.1 to 1.9
- out_weight: bfloat16 [1024, 2048], P('tp'), may hold values from -0.1875 to 0.1875
- ffn_gain: float32 [2048], P('tp'), may hold values from 0.1 to 1.9
- routing: int32 [6144, 2], P(('grp', 'sp')), parts along dimension 0, may hold values from 0 to 15, as said below
- route_weight: float32 [6144, 2], P(('grp', 'sp')), parts along dimension 0, may hold values from 0.2 to 1.2
- expert_gate: bfloat16 [16, 2048, 512], P('sp', None, 'tp'), may hold values from -0.125 to 0.125
- expert_up: bfloat16 [16, 2048, 512], P('sp', None, 'tp'), may hold values from -0.125 to 0.125
- expert_down: bfloat16 [16, 512, 2048], P('sp', None, 'tp'), may hold values from -0.25 to 0.25
- shared_gate: bfloat16 [2048, 512], P(None, 'tp'), may hold values from -0.125 to 0.125
- shared_up: bfloat16 [2048, 512], P(None, 'tp'), may hold values from -0.125 to 0.125
- shared_down: bfloat16 [512, 2048], P(None, 'tp'), may hold values from -0.25 to 0.25
Outputs:
- layer_out: bfloat16 [6144, 2048], P(('grp', 'sp'), 'tp'), parts along dimension 0
The draws below stay inside these ranges and needn't reach their ends.
There are 2 independent parts, one for each index of `grp`. The reference program is written for one: setup_inputs(seed, part) draws one part's arguments, and reference() takes and returns one part's arrays. A program takes and returns all parts, laid end to end along the dimension named above; an argument that names none is the same for every part. Nothing has to cross between parts.
Inputs may be any that keep to these rules, and one draw needn't show every extreme that they name: `routing`: each row names 2 different experts. In each aligned block of 192 rows no expert is named by more than 48 rows, and some expert is named by exactly 48 rows. `doc_ids`: never falls along the sequence; a document holds at most 1536 positions.
All inputs are finite; a program needn't handle non-finite values.
Results may differ from the reference program's by a relative error of at most 0.017.
Values may be sent and summed in bfloat16 or wider, within the bound.
A program may use at most 64 MiB of HBM per device.

```python
import math
import jax
import jax.numpy as jnp
import numpy as np
from jax import lax

D = 2048
D_CONV = 1024
E_H = 512
CONV_K = 3
TOPK = 2
EXP_DEV = 2
TOK_DEV = 384
TOKENS = 3072
EXPERTS = 16
ROWS = 192
MOST = 48
CAP_ALL = 768
DOCS = 4
DOC_MOST = 1536
N_TP = 2


def draw_conv_taps(key, part):
    key_scale = jax.random.fold_in(key, 11)
    key_taps = jax.random.fold_in(key, 12)
    scales = jnp.exp(jax.random.uniform(key_scale, (8,), jnp.float32, minval=-1.1, maxval=1.1))
    taps = jax.random.truncated_normal(key_taps, -3.0, 3.0, (CONV_K, D_CONV), jnp.float32)
    return taps * CONV_K ** (-0.5) * jnp.repeat(scales, D_CONV // 8)[None, :]


def draw_routing(key, part):
    n_dest = EXPERTS // EXP_DEV
    n_source = TOKENS // TOK_DEV
    per_source = TOK_DEV // ROWS
    n_blocks = n_source * per_source
    routes = ROWS * TOPK
    filled = routes // MOST
    dest_iota = jnp.arange(n_dest, dtype=jnp.int32)
    hot_dest = jax.random.randint(jax.random.fold_in(key, 21), (), 0, n_dest, dtype=jnp.int32)
    order_key = jax.random.fold_in(key, 22)

    def source_order(source):
        scores = jax.random.randint(jax.random.fold_in(order_key, source), (n_dest,), 0, 1 << 20, dtype=jnp.int32) * n_dest + dest_iota
        scores = jnp.where(dest_iota == hot_dest, jnp.int32(-1), scores)
        dest_order = jnp.argsort(scores).astype(jnp.int32)
        return (dest_order[:, None] * EXP_DEV + jnp.arange(EXP_DEV, dtype=jnp.int32)[None, :]).reshape(-1)
    orders = jax.vmap(source_order)(jnp.arange(n_source, dtype=jnp.int32))
    position = jnp.arange(routes, dtype=jnp.int32)
    base = filled * MOST
    which = jnp.where(position < base, position // MOST, filled + (position - base) % (EXPERTS - filled))
    listing = orders[:, which]
    listing = jnp.repeat(listing, per_source, axis=0)
    table = jnp.transpose(listing.reshape(n_blocks, TOPK, ROWS), (0, 2, 1))
    perm_key = jax.random.fold_in(key, 23)
    perms = jax.vmap(lambda block: jax.random.permutation(jax.random.fold_in(perm_key, block), ROWS).astype(jnp.int32))(jnp.arange(n_blocks, dtype=jnp.int32))
    table = jnp.take_along_axis(table, perms[:, :, None], axis=1)
    return table.reshape(TOKENS, TOPK).astype(jnp.int32)


def block_levels(stream_key, extent, cuts, least, largest):
    def one(dim, shards_of):
        heights = jax.random.uniform(jax.random.fold_in(jax.random.fold_in(stream_key, 6), dim), (shards_of,), jnp.float32, least / len(cuts), largest / len(cuts))
        return jnp.repeat(jnp.exp(heights), extent[dim] // shards_of).reshape((-1,) + (1,) * (len(extent) - dim - 1))

    gain = one(*cuts[0])
    for cut in cuts[1:]:
        gain = gain * one(*cut)
    return gain


def profile(count, total, most, lean):
    portions = [(1 << 20) // math.isqrt(grade ** lean) + 1 for grade in range(2, count + 1)]
    rest, given = total - most - (count - 1), [1] * (count - 1)
    while rest > 0:
        movable = [i for i in range(count - 1) if given[i] < most]
        mass, left = sum([portions[i] for i in movable]), rest
        for i in movable:
            extra = min(most - given[i], max(1, left * portions[i] // mass), rest)
            given[i] = given[i] + extra
            rest = rest - extra
    return np.array([most] + given)


def uneven(rng, number_of, total, limit, slope):
    if number_of == 2:
        one = jax.random.randint(rng, (), max(1, total - limit), min(limit, total - 1) + 1)
        return jnp.stack([one, total - one])
    lengths = jnp.asarray(profile(number_of, total, limit, slope), jnp.int32)
    couples = (number_of - 1) // 2
    donor, sink = lengths[1:1 + 2 * couples:2], lengths[2:2 + 2 * couples:2]
    margin = jnp.minimum(donor - 1, limit - sink)
    passed = jax.random.randint(jax.random.fold_in(rng, 1), (couples,), 0, 1 << 20) % (margin + 1)
    lengths = lengths.at[1:1 + 2 * couples:2].set(donor - passed).at[2:2 + 2 * couples:2].set(sink + passed)
    return lengths[jax.random.permutation(jax.random.fold_in(rng, 2), number_of)]


def gaussian(stream_key, extent, spread, limit, split=(), held_as=jnp.bfloat16):
    values = spread * jax.random.normal(stream_key, extent, jnp.float32)
    if split:
        values = values * block_levels(stream_key, extent, split, -0.22, 0.18)
    return jnp.clip(values, -limit, limit).astype(held_as)


def setup_inputs(seed: int = 0, part: int = 0) -> dict:
    seeds = jax.random.split(jax.random.key(seed), 18)
    own_keys = jax.random.split(jax.random.fold_in(seeds[17], part), 18)
    out_gate = gaussian(own_keys[0], (TOKENS, D_CONV), 1.0, 6.0, ((0, 8), (1, 2)))
    in_gate = gaussian(own_keys[1], (TOKENS, D_CONV), 1.0, 6.0, ((0, 8), (1, 2)))
    conv_input = gaussian(own_keys[2], (TOKENS, D_CONV), 1.0, 6.0, ((0, 8), (1, 2)))
    doc_ids = jnp.searchsorted(jnp.cumsum(uneven(own_keys[3], DOCS, TOKENS, DOC_MOST, 1)), jnp.arange(TOKENS), side="right").astype(jnp.int32)
    residual = gaussian(own_keys[4], (TOKENS, D), 1.0, 6.0, ((0, 8), (1, 2)))
    conv_taps = draw_conv_taps(jax.random.fold_in(seeds[17], 71), part)
    mix_gain = jnp.clip(1.0 + 0.18 * jax.random.normal(seeds[6], (D_CONV,), jnp.float32), 0.1, 1.9)
    out_weight = gaussian(seeds[7], (D_CONV, D), D_CONV ** -0.5, 0.1875, ((0, 2),))
    ffn_gain = jnp.clip(1.0 + 0.18 * jax.random.normal(seeds[8], (D,), jnp.float32), 0.1, 1.9)
    routing = draw_routing(jax.random.fold_in(jax.random.fold_in(seeds[17], part), 71), part)
    route_weight = jnp.clip(0.2 + 1 * jax.random.uniform(own_keys[10], (TOKENS, TOPK), jnp.float32) ** block_levels(own_keys[10], (TOKENS, TOPK), ((0, 8),), -0.2, 0.2), 0.2, 1.2)
    expert_gate = gaussian(seeds[11], (EXPERTS, D, E_H), D ** -0.5, 0.125, ((0, 8), (2, 2)))
    expert_up = gaussian(seeds[12], (EXPERTS, D, E_H), D ** -0.5, 0.125, ((0, 8), (2, 2)))
    expert_down = gaussian(seeds[13], (EXPERTS, E_H, D), E_H ** -0.5, 0.25, ((0, 8), (2, 2)))
    shared_gate = gaussian(seeds[14], (D, E_H), D ** -0.5, 0.125, ((1, 2),))
    shared_up = gaussian(seeds[15], (D, E_H), D ** -0.5, 0.125, ((1, 2),))
    shared_down = gaussian(seeds[16], (E_H, D), E_H ** -0.5, 0.25, ((1, 2),))
    return dict(out_gate=out_gate, in_gate=in_gate, conv_input=conv_input, doc_ids=doc_ids, residual=residual, conv_taps=conv_taps, mix_gain=mix_gain, out_weight=out_weight, ffn_gain=ffn_gain, routing=routing, route_weight=route_weight, expert_gate=expert_gate, expert_up=expert_up, expert_down=expert_down, shared_gate=shared_gate, shared_up=shared_up, shared_down=shared_down)


def rounded(value):
    return lax.optimization_barrier(value.astype(jnp.bfloat16)).astype(jnp.float32)

def reference(out_gate, in_gate, conv_input, doc_ids, residual, conv_taps, mix_gain, out_weight, ffn_gain, routing, route_weight, expert_gate, expert_up, expert_down, shared_gate, shared_up, shared_down):
    length = out_gate.shape[0]
    product = rounded(in_gate.astype(jnp.float32) * conv_input.astype(jnp.float32))
    extended = jnp.pad(product, ((CONV_K - 1, 0), (0, 0)))
    ext_docs = jnp.pad(doc_ids, (CONV_K - 1, 0), constant_values=-1)
    mixed = jnp.zeros(product.shape, jnp.float32)
    for k in range(CONV_K):
        keep = (ext_docs[k:k + length] == doc_ids)[:, None]
        mixed = mixed + jnp.where(keep, conv_taps[k] * extended[k:k + length], jnp.float32(0.0))
    conv_out = out_gate.astype(jnp.float32) * mixed
    scale = lax.rsqrt(lax.optimization_barrier(jnp.mean(conv_out * conv_out, axis=1, keepdims=True)) + 1e-06)
    normed = (conv_out * scale * mix_gain).astype(jnp.bfloat16)
    width = D_CONV // N_TP
    proj = jnp.zeros((length, D), jnp.float32)
    for block in range(N_TP):
        part = jnp.dot(normed[:, block * width:(block + 1) * width], out_weight[block * width:(block + 1) * width], preferred_element_type=jnp.float32)
        proj = proj + rounded(part)
    stream = (residual.astype(jnp.float32) + proj).astype(jnp.bfloat16)
    stream32 = stream.astype(jnp.float32)
    normal = (stream32 * lax.rsqrt(lax.optimization_barrier(jnp.mean(stream32 * stream32, axis=1, keepdims=True)) + 1e-06) * ffn_gain).astype(jnp.bfloat16)
    shared_hid = (jax.nn.silu(jnp.dot(normal, shared_gate, preferred_element_type=jnp.float32)) * jnp.dot(normal, shared_up, preferred_element_type=jnp.float32)).astype(jnp.bfloat16)
    shared_out = jnp.dot(shared_hid, shared_down, preferred_element_type=jnp.float32)
    padded = jnp.concatenate([normal, jnp.zeros((1, D), jnp.bfloat16)], axis=0)

    def one_expert(expert, total):
        chosen = routing == expert
        weights = lax.optimization_barrier(jnp.sum(jnp.where(chosen, route_weight, jnp.float32(0.0)), axis=1))
        weights = jnp.concatenate([weights, jnp.zeros((1,), jnp.float32)])
        index = jnp.nonzero(jnp.any(chosen, axis=1), size=CAP_ALL, fill_value=length)[0].astype(jnp.int32)
        rows = padded[index]
        gate = jnp.dot(rows, expert_gate[expert], preferred_element_type=jnp.float32)
        upper = jnp.dot(rows, expert_up[expert], preferred_element_type=jnp.float32)
        hid = (jax.nn.silu(gate) * upper).astype(jnp.bfloat16)
        result = jnp.dot(hid, expert_down[expert], preferred_element_type=jnp.float32).astype(jnp.bfloat16)
        return total.at[index].add(weights[index][:, None] * result.astype(jnp.float32))
    routed = lax.fori_loop(0, EXPERTS, one_expert, jnp.zeros((length + 1, D), jnp.float32))
    return (stream32 + shared_out + routed[:length]).astype(jnp.bfloat16)
```

```python
import functools

import jax
import jax.numpy as jnp
from jax import lax
from jax.experimental import pallas as pl
from jax.experimental.pallas import tpu as pltpu
from jax.sharding import PartitionSpec as P

D_CONV = 1024
CONV_K = 3
TOPK = 2
EXP_DEV = 2


def from_behind(value, axis, steps):
    count = lax.axis_size(axis)
    first, last = (max(0, -steps), min(count, count - steps))
    return lax.ppermute(value, axis, [(source, source + steps) for source in range(first, last)])


def body(
    out_gate,
    in_gate,
    conv_input,
    doc_ids,
    residual,
    conv_taps,
    mix_gain,
    out_weight,
    ffn_gain,
    routing,
    route_weight,
    expert_gate,
    expert_up,
    expert_down,
    shared_gate,
    shared_up,
    shared_down,
):
    tokens = residual.shape[0]
    width = out_weight.shape[1]
    n_tp = lax.axis_size("tp")
    n_sp = lax.axis_size("sp")
    rows = tokens // n_tp
    experts = n_sp * EXP_DEV
    most = max(1, 2 * rows * TOPK // experts)
    slots = n_tp * most
    total = experts * slots
    cols = expert_down.shape[2]
    product = (in_gate.astype(jnp.float32) * conv_input.astype(jnp.float32)).astype(jnp.bfloat16)
    tail = (product[tokens - CONV_K + 1 :], doc_ids[tokens - CONV_K + 1 :].astype(jnp.bfloat16))
    prev_rows, prev_docs = from_behind((tail[0], tail[1]), "sp", 1)
    extended = jnp.concatenate([prev_rows, product], axis=0).astype(jnp.float32)
    ext_docs = jnp.concatenate([prev_docs.astype(jnp.int32), doc_ids])
    mixed = jnp.zeros(product.shape, jnp.float32)
    for k in range(CONV_K):
        keep = (ext_docs[k : k + tokens] == doc_ids)[:, None]
        mixed = mixed + jnp.where(keep, conv_taps[k] * extended[k : k + tokens], jnp.float32(0.0))
    conv_out = out_gate.astype(jnp.float32) * mixed
    squares = lax.psum(jnp.sum(conv_out * conv_out, axis=1), "tp")
    normed = (conv_out * lax.rsqrt(squares / D_CONV + 1e-06)[:, None] * mix_gain).astype(
        jnp.bfloat16
    )
    partial_value = jnp.dot(normed, out_weight, preferred_element_type=jnp.float32)
    proj = lax.psum_scatter(
        partial_value.astype(jnp.bfloat16), "tp", scatter_dimension=1, tiled=True
    ).astype(jnp.float32)
    stream = (residual.astype(jnp.float32) + proj).astype(jnp.bfloat16)
    stream32 = stream.astype(jnp.float32)
    stream_sq = lax.psum(jnp.sum(stream32 * stream32, axis=1), "tp")
    normal_cols = (stream32 * lax.rsqrt(stream_sq / width + 1e-06)[:, None] * ffn_gain).astype(
        jnp.bfloat16
    )
    flat_expert = routing.reshape(-1)
    onehot = (flat_expert[:, None] == jnp.arange(experts, dtype=jnp.int32)[None, :]).astype(
        jnp.int32
    )
    blocked = onehot.reshape(n_tp, rows * TOPK, experts)
    earlier = jnp.cumsum(blocked, axis=1) - blocked
    position = jnp.sum(earlier * blocked, axis=2).reshape(-1)
    entry = jnp.arange(tokens * TOPK, dtype=jnp.int32)
    slot = flat_expert * slots + entry // (rows * TOPK) * most + position
    table = jnp.full((total,), tokens, jnp.int32).at[slot].set(entry // TOPK)
    block_rows = lax.all_to_all(normal_cols, "tp", split_axis=0, concat_axis=1, tiled=True)
    mine = lax.dynamic_index_in_dim(
        table.reshape(n_sp, EXP_DEV, n_tp, most), lax.axis_index("tp"), 2, False
    )
    local = jnp.where(mine >= tokens, rows, mine - lax.axis_index("tp") * rows)
    padded_block = jnp.concatenate([block_rows, jnp.zeros((1, width), jnp.bfloat16)], axis=0)
    got = lax.all_to_all(padded_block[local], "sp", split_axis=0, concat_axis=0, tiled=True)
    arrived, whole = (
        lax.all_gather(got, "tp", axis=2, tiled=True),
        lax.all_gather(block_rows.reshape(1, 1, rows, width), "tp", axis=2, tiled=True),
    )
    normal = whole.reshape(tokens, width)
    gate = jnp.einsum("nesd,edh->nesh", arrived, expert_gate, preferred_element_type=jnp.float32)
    upper = jnp.einsum("nesd,edh->nesh", arrived, expert_up, preferred_element_type=jnp.float32)
    hidden = (jax.nn.silu(gate) * upper).astype(jnp.bfloat16)
    hidden_flat = hidden.reshape(n_sp * EXP_DEV * slots, hidden.shape[3])
    shared_hid = (
        jax.nn.silu(jnp.dot(normal, shared_gate, preferred_element_type=jnp.float32))
        * jnp.dot(normal, shared_up, preferred_element_type=jnp.float32)
    ).astype(jnp.bfloat16)
    expert_piece = lax.all_gather(hidden_flat, "tp", axis=1, tiled=True)
    shared_piece = lax.all_gather(shared_hid, "tp", axis=1, tiled=True)
    count = expert_piece.shape[1]
    expert_part = jnp.einsum(
        "nesh,ehd->nesd",
        expert_piece.reshape(n_sp, EXP_DEV, slots, count),
        expert_down,
        preferred_element_type=jnp.float32,
    )
    shared_part = jnp.dot(shared_piece, shared_down, preferred_element_type=jnp.float32)
    returned = lax.all_to_all(
        expert_part.astype(jnp.bfloat16), "sp", split_axis=0, concat_axis=0, tiled=True
    )
    picked = (
        returned.reshape(total, cols)[slot].astype(jnp.float32) * route_weight.reshape(-1)[:, None]
    )
    routed = jnp.sum(picked.reshape(tokens, TOPK, cols), axis=1)
    return (stream32 + shared_part + routed).astype(jnp.bfloat16)


MESH = pl.DeviceIdType.MESH
F32 = jnp.float32
BF16 = jnp.bfloat16


def silu_mul(gate, upper):
    return (gate / (1.0 + jnp.exp(-gate)) * upper).astype(BF16)


def mm(a, b):
    return jnp.dot(a, b, preferred_element_type=F32)


def moe_kernel(
    n_z,
    most,
    own_ref,
    own_meta,
    gain_ref,
    wg,
    wu,
    wd,
    sg,
    su,
    sd,
    out_ref,
    blk,
    meta,
    xs,
    hid,
    shid,
    ys,
    acc,
    outgo,
    sib,
    back,
    fin,
    send_sem,
    recv_sem,
    hid_send,
    hid_recv,
    sh_sem,
    sib_send,
    sib_recv,
    back_send,
    back_recv,
):
    s = lax.axis_index("sp")
    t = lax.axis_index("tp")
    z = s // 2
    c = s % 2
    rows, width = own_ref.shape
    cols = out_ref.shape[2]
    half = wg.shape[2]
    lo = z > 0
    hi = z < n_z - 1
    up, down = {"sp": s + 2}, {"sp": s - 2}
    other, peer = {"sp": s + 1 - 2 * c}, {"tp": 1 - t}
    targets = (up, down, peer, other)

    def slot(zq, cq, tq):
        return (zq * 2 + cq) * 2 + tq

    def zone(i):
        return z + (1 - 2 * (i % 2)) * ((i + 1) // 2)

    def valid(i):
        zq = zone(i)
        return (i >= 0) & (i <= 2 * n_z - 2) & (zq >= 0) & (zq < n_z)

    def remote(src, dst, ssem, rsem, dev):
        return pltpu.make_async_remote_copy(
            src_ref=src,
            dst_ref=dst,
            send_sem=ssem,
            recv_sem=rsem,
            device_id=dev,
            device_id_type=MESH,
        )

    def block(b, way, own=False):
        return (
            remote(
                own_ref if own else blk.at[b],
                blk.at[b],
                send_sem.at[way, b, 0],
                recv_sem.at[b, 0],
                targets[way],
            ),
            remote(
                own_meta if own else meta.at[b],
                meta.at[b],
                send_sem.at[way, b, 1],
                recv_sem.at[b, 1],
                targets[way],
            ),
        )

    def start(b, way, own=False):
        for copy in block(b, way, own):
            copy.start()

    def arrived(b):
        for copy in block(b, 2):
            copy.wait_recv()

    def hid_copy(zq):
        return remote(hid.at[t, zq], hid.at[t, zq], hid_send.at[zq], hid_recv.at[zq], peer)

    def sh_copy():
        return remote(shid.at[t], shid.at[t], sh_sem.at[0], sh_sem.at[1], peer)

    def sib_copy(zq):
        return remote(outgo.at[zq], sib.at[zq], sib_send.at[zq], sib_recv.at[zq], other)

    def back_copy(zq, tq, to, dev):
        return remote(
            acc.at[zq, tq],
            back.at[to, tq],
            back_send.at[zq, tq],
            back_recv.at[to, tq],
            dev,
        )

    barrier = pltpu.get_barrier_semaphore()
    for way, there in ((0, hi), (1, lo)):

        @pl.when(there)
        def _():
            pl.semaphore_signal(barrier, inc=1, device_id=targets[way], device_id_type=MESH)

    for way in (2, 3):
        pl.semaphore_signal(barrier, inc=1, device_id=targets[way], device_id_type=MESH)
    pl.semaphore_wait(barrier, 2 + lo.astype(jnp.int32) + hi.astype(jnp.int32))

    mine = slot(z, c, t)

    @pl.when(hi)
    def _():
        start(mine, 0, True)

    @pl.when(lo)
    def _():
        start(mine, 1, True)

    start(mine, 2, True)
    start(mine, 3, True)
    blk[mine] = own_ref[...]
    meta[mine] = own_meta[...]

    def picks(b):
        pair = meta[b, z][:, :rows]
        info = jnp.where(c == 0, pair[: 2 * EXP_DEV], pair[2 * EXP_DEV :])
        place = lax.broadcasted_iota(jnp.int32, (most, rows), 0).astype(F32)
        return info, [(info[e : e + 1] == place).astype(F32) for e in range(EXP_DEV)]

    def normalise(value):
        ms = jnp.mean(value * value, axis=1, keepdims=True)
        return (value * lax.rsqrt(ms + 1e-06) * gain_ref[...]).astype(BF16)

    def group(j):
        return [(p, tq, c + p - 2 * c * p) for p in range(2) for tq in range(2)]

    def hidden(zq):
        for j, (p, tq, cq) in enumerate(group(zq)):
            b = slot(zq, cq, tq)
            _, chosen = picks(b)
            sel = jnp.concatenate(chosen, axis=0).astype(BF16)
            got = normalise(mm(sel, blk[b]))
            for e in range(EXP_DEV):
                xs[e, j * most : (j + 1) * most, :] = got[e * most : (e + 1) * most]
        for e in range(EXP_DEV):
            hid[t, zq, e] = silu_mul(mm(xs[e], wg[e]), mm(xs[e], wu[e]))

    @pl.loop(1, 2 * n_z + 1)
    def _(i):
        @pl.when(valid(i))
        def _():
            zq = zone(i)
            b = slot(zq, c, t)
            arrived(b)

            @pl.when(hi & (zq < z))
            def _():
                start(b, 0)

            @pl.when(lo & (zq > z))
            def _():
                start(b, 1)

            start(b, 2)
            start(b, 3)

        @pl.when(valid(i - 2))
        def _():
            zq = zone(i - 2)
            b = slot(zq, c, 1 - t)
            arrived(b)
            start(b, 3)
            arrived(slot(zq, 1 - c, t))
            arrived(slot(zq, 1 - c, 1 - t))
            hidden(zq)
            hid_copy(zq).start()

    for tq in range(2):
        whole = normalise(blk[slot(z, c, tq)].astype(F32))
        shid[t, tq] = silu_mul(mm(whole, sg[...]), mm(whole, su[...]))
    sh_copy().start()

    @pl.loop(0, 2 * n_z - 1)
    def _(k):
        i = 2 * n_z - 2 - k

        @pl.when(valid(i))
        def _():
            zq = zone(i)
            hid_copy(zq).wait_recv()
            for e in range(EXP_DEV):
                ys[e] = (
                    mm(hid[0, zq, e], wd[e, :half, :]) + mm(hid[1, zq, e], wd[e, half:, :])
                ).astype(BF16)
            for j, (p, tq, cq) in enumerate(group(zq)):
                info, chosen = picks(slot(zq, cq, tq))
                parts = []
                for e in range(EXP_DEV):
                    weight = jnp.sum(
                        chosen[e] * info[EXP_DEV + e : EXP_DEV + e + 1], axis=1, keepdims=True
                    )
                    part = ys[e, j * most : (j + 1) * most, :].astype(F32)
                    parts.append((part * weight).astype(BF16))
                sel = jnp.concatenate(chosen, axis=0).astype(BF16)
                spread = lax.dot_general(
                    sel,
                    jnp.concatenate(parts, axis=0),
                    (((0,), (0,)), ((), ())),
                    preferred_element_type=F32,
                ).astype(BF16)
                if p == 0:
                    acc[zq, tq] = spread
                else:
                    outgo[zq, tq] = spread
            sib_copy(zq).start()

    @pl.loop(0, 2 * n_z - 2)
    def _(k):
        i = 2 * n_z - 2 - k

        @pl.when(valid(i))
        def _():
            zq = zone(i)
            sib_copy(zq).wait_recv()
            rising = zq > z
            more = (rising & lo) | (jnp.logical_not(rising) & hi)
            for tq in range(2):
                both = acc[zq, tq].astype(F32) + sib[zq, tq].astype(F32)

                @pl.when(more)
                def _():
                    back_copy(zq, tq, zq, up).wait_recv()
                    acc[zq, tq] = (both + back[zq, tq].astype(F32)).astype(BF16)

                @pl.when(jnp.logical_not(more))
                def _():
                    acc[zq, tq] = both.astype(BF16)

                @pl.when(rising)
                def _():
                    back_copy(zq, tq, zq, up).start()

                @pl.when(zq < z - 1)
                def _():
                    back_copy(zq, tq, zq, down).start()

                @pl.when(zq == z - 1)
                def _():
                    back_copy(zq, tq, n_z, down).start()

    sib_copy(z).wait_recv()
    sh_copy().wait_recv()
    for tq in range(2):
        stream = blk[slot(z, c, tq), :, pl.ds(pl.multiple_of(t * cols, cols), cols)]
        fin[tq] = (
            stream.astype(F32)
            + mm(shid[0, tq], sd[:half, :])
            + mm(shid[1, tq], sd[half:, :])
            + acc[z, tq].astype(F32)
            + sib[z, tq].astype(F32)
        )
    for tq in range(2):

        @pl.when(lo)
        def _():
            back_copy(z, tq, z, up).wait_recv()
            fin[tq] = fin[tq] + back[z, tq].astype(F32)

        @pl.when(hi)
        def _():
            back_copy(z, tq, n_z, up).wait_recv()
            fin[tq] = fin[tq] + back[n_z, tq].astype(F32)

        out_ref[tq] = fin[tq].astype(BF16)

    @pl.loop(0, n_z)
    def _(zq):
        b = slot(zq, c, t)

        @pl.when(hi & (zq <= z))
        def _():
            for copy in block(b, 0):
                copy.wait_send()

        @pl.when(lo & (zq >= z))
        def _():
            for copy in block(b, 1):
                copy.wait_send()

        for copy in block(b, 2) + block(b, 3) + block(slot(zq, c, 1 - t), 3):
            copy.wait_send()
        hid_copy(zq).wait_send()
        sib_copy(zq).wait_send()

        @pl.when(zq != z)
        def _():
            for tq in range(2):
                back_copy(zq, tq, zq, up).wait_send()

    sh_copy().wait_send()


def fast(
    out_gate,
    in_gate,
    conv_input,
    doc_ids,
    residual,
    conv_taps,
    mix_gain,
    out_weight,
    ffn_gain,
    routing,
    route_weight,
    expert_gate,
    expert_up,
    expert_down,
    shared_gate,
    shared_up,
    shared_down,
):
    tokens, cols = residual.shape
    width = out_weight.shape[1]
    n_tp, n_sp = lax.axis_size("tp"), lax.axis_size("sp")
    n_z = n_sp // 2
    rows = tokens // n_tp
    experts = n_sp * EXP_DEV
    most = max(1, 2 * rows * TOPK // experts)
    t = lax.axis_index("tp")
    swap = [(0, 1), (1, 0)]

    def cut(value, who):
        return lax.dynamic_slice_in_dim(value, who * rows, rows, 0)

    res_other = lax.ppermute(cut(residual, 1 - t), "tp", swap)
    product = (in_gate.astype(F32) * conv_input.astype(F32)).astype(BF16)
    prev_rows, prev_docs = from_behind(
        (product[tokens - CONV_K + 1 :], doc_ids[tokens - CONV_K + 1 :].astype(BF16)), "sp", 1
    )
    extended = jnp.concatenate([prev_rows, product], axis=0).astype(F32)
    ext_docs = jnp.concatenate([prev_docs.astype(jnp.int32), doc_ids])
    mixed = jnp.zeros(product.shape, F32)
    for k in range(CONV_K):
        keep = (ext_docs[k : k + tokens] == doc_ids)[:, None]
        mixed = mixed + jnp.where(keep, conv_taps[k] * extended[k : k + tokens], F32(0.0))
    conv_out = out_gate.astype(F32) * mixed
    sums = jnp.sum(conv_out * conv_out, axis=1)
    sums_other = lax.ppermute(sums, "tp", swap)
    gain_other = lax.ppermute(ffn_gain, "tp", swap)
    squares = sums + sums_other
    first = t == 0
    gain = jnp.concatenate(
        [jnp.where(first, ffn_gain, gain_other), jnp.where(first, gain_other, ffn_gain)]
    )
    normed = (conv_out * lax.rsqrt(squares / D_CONV + 1e-06)[:, None] * mix_gain).astype(BF16)
    given = mm(cut(normed, 1 - t), out_weight).astype(BF16)
    taken = lax.ppermute(given, "tp", swap)
    kept = mm(cut(normed, t), out_weight).astype(BF16)
    res_mine = cut(residual, t)
    res = jnp.concatenate(
        [jnp.where(first, res_mine, res_other), jnp.where(first, res_other, res_mine)], axis=1
    )
    stream = (res.astype(F32) + (kept.astype(F32) + taken.astype(F32))).astype(BF16)

    names = cut(routing, t)
    weights = cut(route_weight, t)
    hot = names[:, :, None] == jnp.arange(experts, dtype=jnp.int32)
    named = jnp.any(hot, axis=1)
    placed = jnp.sum(jnp.where(hot, weights[:, :, None], F32(0.0)), axis=1)
    before = jnp.arange(rows)[:, None] > jnp.arange(rows)[None, :]
    earlier = mm(before.astype(BF16), named.astype(BF16))
    position = jnp.where(named, earlier, F32(-1.0))
    info = jnp.stack([position, placed], axis=0).reshape(2, rows, n_sp, EXP_DEV)
    info = info.transpose(2, 0, 3, 1).reshape(n_z, 4 * EXP_DEV, rows)
    pad = -rows % 128
    info = jnp.pad(info, ((0, 0), (0, 0), (0, pad)), constant_values=-1.0)

    blocks = n_sp * n_tp
    half = expert_gate.shape[2]
    vm = pl.BlockSpec(memory_space=pltpu.VMEM)
    dma = pltpu.SemaphoreType.DMA
    out = pl.pallas_call(
        functools.partial(moe_kernel, n_z, most),
        out_shape=jax.ShapeDtypeStruct((n_tp, rows, cols), BF16),
        in_specs=[vm] * 9,
        out_specs=vm,
        scratch_shapes=[
            pltpu.VMEM((blocks, rows, width), BF16),
            pltpu.VMEM((blocks,) + info.shape, F32),
            pltpu.VMEM((EXP_DEV, 4 * most, width), BF16),
            pltpu.VMEM((2, n_z, EXP_DEV, 4 * most, half), BF16),
            pltpu.VMEM((2, 2, rows, half), BF16),
            pltpu.VMEM((EXP_DEV, 4 * most, cols), BF16),
            pltpu.VMEM((n_z, 2, rows, cols), BF16),
            pltpu.VMEM((n_z, 2, rows, cols), BF16),
            pltpu.VMEM((n_z, 2, rows, cols), BF16),
            pltpu.VMEM((n_z + 1, 2, rows, cols), BF16),
            pltpu.VMEM((2, rows, cols), F32),
            dma((4, blocks, 2)),
            dma((blocks, 2)),
            dma((n_z,)),
            dma((n_z,)),
            dma((2,)),
            dma((n_z,)),
            dma((n_z,)),
            dma((n_z, 2)),
            dma((n_z + 1, 2)),
        ],
        compiler_params=pltpu.CompilerParams(
            collective_id=0, has_side_effects=True, vmem_limit_bytes=64 * 1024 * 1024 - 65536
        ),
    )(
        stream,
        info,
        gain[None, :],
        expert_gate,
        expert_up,
        expert_down,
        shared_gate,
        shared_up,
        shared_down,
    )
    return out.reshape(tokens, cols)


def fits(mesh):
    return mesh.shape["tp"] == 2 and mesh.shape["sp"] in (4, 6, 8)


def solution(mesh):
    return jax.shard_map(
        fast if fits(mesh) else body,
        mesh=mesh,
        in_specs=(
            P(("grp", "sp"), "tp"),
            P(("grp", "sp"), "tp"),
            P(("grp", "sp"), "tp"),
            P(("grp", "sp")),
            P(("grp", "sp"), "tp"),
            P(None, "tp"),
            P("tp"),
            P("tp", None),
            P("tp"),
            P(("grp", "sp"), None),
            P(("grp", "sp"), None),
            P("sp", None, "tp"),
            P("sp", None, "tp"),
            P("sp", None, "tp"),
            P(None, "tp"),
            P(None, "tp"),
            P(None, "tp"),
        ),
        out_specs=P(("grp", "sp"), "tp"),
        check_vma=False,
    )
```

```python
import functools

import jax
import jax.numpy as jnp
from jax import lax
from jax.experimental import pallas as pl
from jax.experimental.pallas import tpu as pltpu
from jax.sharding import PartitionSpec as P

D_CONV = 1024
CONV_K = 3
TOPK = 2
EXP_DEV = 2


def from_behind(value, axis, steps):
    count = lax.axis_size(axis)
    first, last = (max(0, -steps), min(count, count - steps))
    return lax.ppermute(value, axis, [(source, source + steps) for source in range(first, last)])


def body(
    out_gate,
    in_gate,
    conv_input,
    doc_ids,
    residual,
    conv_taps,
    mix_gain,
    out_weight,
    ffn_gain,
    routing,
    route_weight,
    expert_gate,
    expert_up,
    expert_down,
    shared_gate,
    shared_up,
    shared_down,
):
    tokens = residual.shape[0]
    width = out_weight.shape[1]
    n_tp = lax.axis_size("tp")
    n_sp = lax.axis_size("sp")
    rows = tokens // n_tp
    experts = n_sp * EXP_DEV
    most = max(1, 2 * rows * TOPK // experts)
    slots = n_tp * most
    total = experts * slots
    cols = expert_down.shape[2]
    product = (in_gate.astype(jnp.float32) * conv_input.astype(jnp.float32)).astype(jnp.bfloat16)
    tail = (product[tokens - CONV_K + 1 :], doc_ids[tokens - CONV_K + 1 :].astype(jnp.bfloat16))
    prev_rows, prev_docs = from_behind((tail[0], tail[1]), "sp", 1)
    extended = jnp.concatenate([prev_rows, product], axis=0).astype(jnp.float32)
    ext_docs = jnp.concatenate([prev_docs.astype(jnp.int32), doc_ids])
    mixed = jnp.zeros(product.shape, jnp.float32)
    for k in range(CONV_K):
        keep = (ext_docs[k : k + tokens] == doc_ids)[:, None]
        mixed = mixed + jnp.where(keep, conv_taps[k] * extended[k : k + tokens], jnp.float32(0.0))
    conv_out = out_gate.astype(jnp.float32) * mixed
    squares = lax.psum(jnp.sum(conv_out * conv_out, axis=1), "tp")
    normed = (conv_out * lax.rsqrt(squares / D_CONV + 1e-06)[:, None] * mix_gain).astype(
        jnp.bfloat16
    )
    partial_value = jnp.dot(normed, out_weight, preferred_element_type=jnp.float32)
    proj = lax.psum_scatter(
        partial_value.astype(jnp.bfloat16), "tp", scatter_dimension=1, tiled=True
    ).astype(jnp.float32)
    stream = (residual.astype(jnp.float32) + proj).astype(jnp.bfloat16)
    stream32 = stream.astype(jnp.float32)
    stream_sq = lax.psum(jnp.sum(stream32 * stream32, axis=1), "tp")
    normal_cols = (stream32 * lax.rsqrt(stream_sq / width + 1e-06)[:, None] * ffn_gain).astype(
        jnp.bfloat16
    )
    flat_expert = routing.reshape(-1)
    onehot = (flat_expert[:, None] == jnp.arange(experts, dtype=jnp.int32)[None, :]).astype(
        jnp.int32
    )
    blocked = onehot.reshape(n_tp, rows * TOPK, experts)
    earlier = jnp.cumsum(blocked, axis=1) - blocked
    position = jnp.sum(earlier * blocked, axis=2).reshape(-1)
    entry = jnp.arange(tokens * TOPK, dtype=jnp.int32)
    slot = flat_expert * slots + entry // (rows * TOPK) * most + position
    table = jnp.full((total,), tokens, jnp.int32).at[slot].set(entry // TOPK)
    block_rows = lax.all_to_all(normal_cols, "tp", split_axis=0, concat_axis=1, tiled=True)
    mine = lax.dynamic_index_in_dim(
        table.reshape(n_sp, EXP_DEV, n_tp, most), lax.axis_index("tp"), 2, False
    )
    local = jnp.where(mine >= tokens, rows, mine - lax.axis_index("tp") * rows)
    padded_block = jnp.concatenate([block_rows, jnp.zeros((1, width), jnp.bfloat16)], axis=0)
    got = lax.all_to_all(padded_block[local], "sp", split_axis=0, concat_axis=0, tiled=True)
    arrived, whole = (
        lax.all_gather(got, "tp", axis=2, tiled=True),
        lax.all_gather(block_rows.reshape(1, 1, rows, width), "tp", axis=2, tiled=True),
    )
    normal = whole.reshape(tokens, width)
    gate = jnp.einsum("nesd,edh->nesh", arrived, expert_gate, preferred_element_type=jnp.float32)
    upper = jnp.einsum("nesd,edh->nesh", arrived, expert_up, preferred_element_type=jnp.float32)
    hidden = (jax.nn.silu(gate) * upper).astype(jnp.bfloat16)
    hidden_flat = hidden.reshape(n_sp * EXP_DEV * slots, hidden.shape[3])
    shared_hid = (
        jax.nn.silu(jnp.dot(normal, shared_gate, preferred_element_type=jnp.float32))
        * jnp.dot(normal, shared_up, preferred_element_type=jnp.float32)
    ).astype(jnp.bfloat16)
    expert_piece = lax.all_gather(hidden_flat, "tp", axis=1, tiled=True)
    shared_piece = lax.all_gather(shared_hid, "tp", axis=1, tiled=True)
    count = expert_piece.shape[1]
    expert_part = jnp.einsum(
        "nesh,ehd->nesd",
        expert_piece.reshape(n_sp, EXP_DEV, slots, count),
        expert_down,
        preferred_element_type=jnp.float32,
    )
    shared_part = jnp.dot(shared_piece, shared_down, preferred_element_type=jnp.float32)
    returned = lax.all_to_all(
        expert_part.astype(jnp.bfloat16), "sp", split_axis=0, concat_axis=0, tiled=True
    )
    picked = (
        returned.reshape(total, cols)[slot].astype(jnp.float32) * route_weight.reshape(-1)[:, None]
    )
    routed = jnp.sum(picked.reshape(tokens, TOPK, cols), axis=1)
    return (stream32 + shared_part + routed).astype(jnp.bfloat16)


MESH = pl.DeviceIdType.MESH
F32 = jnp.float32
BF16 = jnp.bfloat16


def silu_mul(gate, upper):
    return (gate / (1.0 + jnp.exp(-gate)) * upper).astype(BF16)


def mm(a, b):
    return jnp.dot(a, b, preferred_element_type=F32)


def moe_kernel(
    n_z,
    most,
    own_ref,
    own_meta,
    gain_ref,
    wg_hbm,
    wu_hbm,
    wd_hbm,
    sg_hbm,
    su_hbm,
    sd_hbm,
    out_ref,
    wg,
    wu,
    wd,
    sg,
    su,
    sd,
    blk,
    meta,
    xs,
    hid,
    shid,
    ys,
    acc,
    outgo,
    sib,
    back,
    fin,
    send_sem,
    recv_sem,
    hid_send,
    hid_recv,
    sh_sem,
    sib_send,
    sib_recv,
    back_send,
    back_recv,
    load_sem,
):
    loads = [
        pltpu.make_async_copy(src, dst, load_sem.at[n])
        for n, (src, dst) in enumerate(
            (
                (wg_hbm, wg),
                (wu_hbm, wu),
                (sg_hbm, sg),
                (su_hbm, su),
                (wd_hbm, wd),
                (sd_hbm, sd),
            )
        )
    ]
    for load in loads:
        load.start()
    s = lax.axis_index("sp")
    t = lax.axis_index("tp")
    z = s // 2
    c = s % 2
    rows, width = own_ref.shape
    cols = out_ref.shape[2]
    half = wg.shape[2]
    per, piece = acc.shape[1] // 2, acc.shape[2]
    lo = z > 0
    hi = z < n_z - 1
    up, down = {"sp": s + 2}, {"sp": s - 2}
    other, peer = {"sp": s + 1 - 2 * c}, {"tp": 1 - t}
    targets = (up, down, peer, other)

    def slot(zq, cq, tq):
        return (zq * 2 + cq) * 2 + tq

    def zone(i):
        return z + (1 - 2 * (i % 2)) * ((i + 1) // 2)

    def valid(i):
        zq = zone(i)
        return (i >= 0) & (i <= 2 * n_z - 2) & (zq >= 0) & (zq < n_z)

    def remote(src, dst, ssem, rsem, dev):
        return pltpu.make_async_remote_copy(
            src_ref=src,
            dst_ref=dst,
            send_sem=ssem,
            recv_sem=rsem,
            device_id=dev,
            device_id_type=MESH,
        )

    def block(b, way, own=False):
        return (
            remote(
                own_ref if own else blk.at[b],
                blk.at[b],
                send_sem.at[way, b, 0],
                recv_sem.at[b, 0],
                targets[way],
            ),
            remote(
                own_meta if own else meta.at[b],
                meta.at[b],
                send_sem.at[way, b, 1],
                recv_sem.at[b, 1],
                targets[way],
            ),
        )

    def start(b, way, own=False):
        for copy in block(b, way, own):
            copy.start()

    def arrived(b):
        for copy in block(b, 2):
            copy.wait_recv()

    def hid_copy(zq):
        return remote(hid.at[t, zq], hid.at[t, zq], hid_send.at[zq], hid_recv.at[zq], peer)

    def sh_copy():
        return remote(shid.at[t], shid.at[t], sh_sem.at[0], sh_sem.at[1], peer)

    def sib_copy(zq):
        return remote(outgo.at[zq], sib.at[zq], sib_send.at[zq], sib_recv.at[zq], other)

    def back_copy(zq, q, to, dev):
        return remote(
            acc.at[zq, q],
            back.at[to, q],
            back_send.at[zq, q],
            back_recv.at[to, q],
            dev,
        )

    def pass_on(zq, q):
        @pl.when(zq > z)
        def _():
            back_copy(zq, q, zq, up).start()

        @pl.when(zq < z - 1)
        def _():
            back_copy(zq, q, zq, down).start()

        @pl.when(zq == z - 1)
        def _():
            back_copy(zq, q, n_z, down).start()

    barrier = pltpu.get_barrier_semaphore()
    for way, there in ((0, hi), (1, lo)):

        @pl.when(there)
        def _():
            pl.semaphore_signal(barrier, inc=1, device_id=targets[way], device_id_type=MESH)

    for way in (2, 3):
        pl.semaphore_signal(barrier, inc=1, device_id=targets[way], device_id_type=MESH)
    pl.semaphore_wait(barrier, 2 + lo.astype(jnp.int32) + hi.astype(jnp.int32))

    mine = slot(z, c, t)

    @pl.when(hi)
    def _():
        start(mine, 0, True)

    @pl.when(lo)
    def _():
        start(mine, 1, True)

    start(mine, 2, True)
    start(mine, 3, True)
    blk[mine] = own_ref[...]
    meta[mine] = own_meta[...]

    def picks(b):
        pair = meta[b, z][:, :rows]
        info = jnp.where(c == 0, pair[: 2 * EXP_DEV], pair[2 * EXP_DEV :])
        place = lax.broadcasted_iota(jnp.int32, (most, rows), 0).astype(F32)
        return info, [(info[e : e + 1] == place).astype(F32) for e in range(EXP_DEV)]

    def normalise(value):
        ms = jnp.mean(value * value, axis=1, keepdims=True)
        return (value * lax.rsqrt(ms + 1e-06) * gain_ref[...]).astype(BF16)

    def group(j):
        return [(p, tq, c + p - 2 * c * p) for p in range(2) for tq in range(2)]

    def hidden(zq):
        for j, (p, tq, cq) in enumerate(group(zq)):
            b = slot(zq, cq, tq)
            _, chosen = picks(b)
            sel = jnp.concatenate(chosen, axis=0).astype(BF16)
            got = normalise(mm(sel, blk[b]))
            for e in range(EXP_DEV):
                xs[e, j * most : (j + 1) * most, :] = got[e * most : (e + 1) * most]
        for e in range(EXP_DEV):
            hid[t, zq, e] = silu_mul(mm(xs[e], wg[e]), mm(xs[e], wu[e]))

    def shared():
        for tq in range(2):
            whole = normalise(blk[slot(z, c, tq)].astype(F32))
            shid[t, tq] = silu_mul(mm(whole, sg[...]), mm(whole, su[...]))

    def results(zq):
        hid_copy(zq).wait_recv()
        for e in range(EXP_DEV):
            ys[e] = (
                mm(hid[0, zq, e], wd[e, :half, :]) + mm(hid[1, zq, e], wd[e, half:, :])
            ).astype(BF16)
        for j, (p, tq, cq) in enumerate(group(zq)):
            info, chosen = picks(slot(zq, cq, tq))
            parts = []
            for e in range(EXP_DEV):
                weight = jnp.sum(
                    chosen[e] * info[EXP_DEV + e : EXP_DEV + e + 1], axis=1, keepdims=True
                )
                part = ys[e, j * most : (j + 1) * most, :].astype(F32)
                parts.append((part * weight).astype(BF16))
            sel = jnp.concatenate(chosen, axis=0).astype(BF16)
            spread = lax.dot_general(
                sel,
                jnp.concatenate(parts, axis=0),
                (((0,), (0,)), ((), ())),
                preferred_element_type=F32,
            ).astype(BF16)
            into = acc if p == 0 else outgo
            for h in range(per):
                into[zq, tq * per + h] = spread[h * piece : (h + 1) * piece]
        sib_copy(zq).start()

    def is_end(zq):
        return ((zq > z) & jnp.logical_not(lo)) | ((zq < z) & jnp.logical_not(hi))

    for load in loads[:2]:
        load.wait()

    @pl.loop(1, 2 * n_z + 3)
    def _(i):
        @pl.when(valid(i))
        def _():
            zq = zone(i)
            b = slot(zq, c, t)
            arrived(b)

            @pl.when(hi & (zq < z))
            def _():
                start(b, 0)

            @pl.when(lo & (zq > z))
            def _():
                start(b, 1)

            start(b, 2)
            start(b, 3)

        @pl.when(valid(i - 2))
        def _():
            zq = zone(i - 2)
            b = slot(zq, c, 1 - t)
            arrived(b)
            start(b, 3)
            arrived(slot(zq, 1 - c, t))
            arrived(slot(zq, 1 - c, 1 - t))
            hidden(zq)
            hid_copy(zq).start()

        @pl.when(i == 3)
        def _():
            for load in loads[2:]:
                load.wait()
            shared()

        @pl.when(i == 2 * n_z)
        def _():
            sh_copy().start()

        @pl.when(valid(i - 4))
        def _():
            zq = zone(i - 4)
            results(zq)

            @pl.when(is_end(zq))
            def _():
                sib_copy(zq).wait_recv()
                for q in range(2 * per):
                    acc[zq, q] = (acc[zq, q].astype(F32) + sib[zq, q].astype(F32)).astype(BF16)
                    pass_on(zq, q)

    above = n_z - 1 - z
    up_first = (above >= z).astype(jnp.int32)

    @pl.loop(0, n_z - 1)
    def _(k):
        in_up = (k < above).astype(jnp.int32)
        in_down = (k < z).astype(jnp.int32)
        rise = in_up * (z + 1 + k) + (1 - in_up) * (z - 1 - (k - above))
        fall = in_down * (z - 1 - k) + (1 - in_down) * (z + 1 + (k - z))
        zq = up_first * rise + (1 - up_first) * fall

        @pl.when(jnp.logical_not(is_end(zq)))
        def _():
            sib_copy(zq).wait_recv()
            for q in range(2 * per):
                back_copy(zq, q, zq, up).wait_recv()
                acc[zq, q] = (
                    acc[zq, q].astype(F32) + sib[zq, q].astype(F32) + back[zq, q].astype(F32)
                ).astype(BF16)
                pass_on(zq, q)

    sib_copy(z).wait_recv()
    sh_copy().wait_recv()
    for tq in range(2):
        stream = blk[slot(z, c, tq), :, pl.ds(pl.multiple_of(t * cols, cols), cols)]
        base = (
            stream.astype(F32)
            + mm(shid[0, tq], sd[:half, :])
            + mm(shid[1, tq], sd[half:, :])
        )
        for h in range(per):
            q = tq * per + h
            fin[q] = (
                base[h * piece : (h + 1) * piece]
                + acc[z, q].astype(F32)
                + sib[z, q].astype(F32)
            )
    for q in range(2 * per):

        @pl.when(lo)
        def _():
            back_copy(z, q, z, up).wait_recv()
            fin[q] = fin[q] + back[z, q].astype(F32)

        @pl.when(hi)
        def _():
            back_copy(z, q, n_z, up).wait_recv()
            fin[q] = fin[q] + back[n_z, q].astype(F32)

        tq, h = divmod(q, per)
        out_ref[tq, h * piece : (h + 1) * piece, :] = fin[q].astype(BF16)

    @pl.loop(0, n_z)
    def _(zq):
        b = slot(zq, c, t)

        @pl.when(hi & (zq <= z))
        def _():
            for copy in block(b, 0):
                copy.wait_send()

        @pl.when(lo & (zq >= z))
        def _():
            for copy in block(b, 1):
                copy.wait_send()

        for copy in block(b, 2) + block(b, 3) + block(slot(zq, c, 1 - t), 3):
            copy.wait_send()
        hid_copy(zq).wait_send()
        sib_copy(zq).wait_send()

        @pl.when(zq != z)
        def _():
            for q in range(2 * per):
                back_copy(zq, q, zq, up).wait_send()

    sh_copy().wait_send()


def fast(
    out_gate,
    in_gate,
    conv_input,
    doc_ids,
    residual,
    conv_taps,
    mix_gain,
    out_weight,
    ffn_gain,
    routing,
    route_weight,
    expert_gate,
    expert_up,
    expert_down,
    shared_gate,
    shared_up,
    shared_down,
):
    tokens, cols = residual.shape
    width = out_weight.shape[1]
    n_tp, n_sp = lax.axis_size("tp"), lax.axis_size("sp")
    n_z = n_sp // 2
    rows = tokens // n_tp
    experts = n_sp * EXP_DEV
    most = max(1, 2 * rows * TOPK // experts)
    t = lax.axis_index("tp")
    swap = [(0, 1), (1, 0)]

    def cut(value, who):
        return lax.dynamic_slice_in_dim(value, who * rows, rows, 0)

    res_other = lax.ppermute(cut(residual, 1 - t), "tp", swap)
    product = (in_gate.astype(F32) * conv_input.astype(F32)).astype(BF16)
    prev_rows, prev_docs = from_behind(
        (product[tokens - CONV_K + 1 :], doc_ids[tokens - CONV_K + 1 :].astype(BF16)), "sp", 1
    )
    extended = jnp.concatenate([prev_rows, product], axis=0).astype(F32)
    ext_docs = jnp.concatenate([prev_docs.astype(jnp.int32), doc_ids])
    mixed = jnp.zeros(product.shape, F32)
    for k in range(CONV_K):
        keep = (ext_docs[k : k + tokens] == doc_ids)[:, None]
        mixed = mixed + jnp.where(keep, conv_taps[k] * extended[k : k + tokens], F32(0.0))
    conv_out = out_gate.astype(F32) * mixed
    sums = jnp.sum(conv_out * conv_out, axis=1)
    sums_other = lax.ppermute(sums, "tp", swap)
    gain_other = lax.ppermute(ffn_gain, "tp", swap)
    squares = sums + sums_other
    first = t == 0
    gain = jnp.concatenate(
        [jnp.where(first, ffn_gain, gain_other), jnp.where(first, gain_other, ffn_gain)]
    )
    normed = (conv_out * lax.rsqrt(squares / D_CONV + 1e-06)[:, None] * mix_gain).astype(BF16)
    given = mm(cut(normed, 1 - t), out_weight).astype(BF16)
    taken = lax.ppermute(given, "tp", swap)
    kept = lax.optimization_barrier(mm(cut(normed, t), out_weight).astype(BF16))
    res_mine = cut(residual, t)
    res = jnp.concatenate(
        [jnp.where(first, res_mine, res_other), jnp.where(first, res_other, res_mine)], axis=1
    )
    stream = (res.astype(F32) + (kept.astype(F32) + taken.astype(F32))).astype(BF16)

    names = cut(routing, t)
    weights = cut(route_weight, t)
    hot = names[:, :, None] == jnp.arange(experts, dtype=jnp.int32)
    named = jnp.any(hot, axis=1)
    placed = jnp.sum(jnp.where(hot, weights[:, :, None], F32(0.0)), axis=1)
    before = jnp.arange(rows)[:, None] > jnp.arange(rows)[None, :]
    earlier = mm(before.astype(BF16), named.astype(BF16))
    position = jnp.where(named, earlier, F32(-1.0))
    info = jnp.stack([position, placed], axis=0).reshape(2, rows, n_sp, EXP_DEV)
    info = info.transpose(2, 0, 3, 1).reshape(n_z, 4 * EXP_DEV, rows)
    pad = -rows % 128
    info = jnp.pad(info, ((0, 0), (0, 0), (0, pad)), constant_values=-1.0)

    per = 2
    piece = rows // per
    blocks = n_sp * n_tp
    half = expert_gate.shape[2]
    vm = pl.BlockSpec(memory_space=pltpu.VMEM)
    dma = pltpu.SemaphoreType.DMA
    out = pl.pallas_call(
        functools.partial(moe_kernel, n_z, most),
        out_shape=jax.ShapeDtypeStruct((n_tp, rows, cols), BF16),
        in_specs=[vm] * 3 + [pl.BlockSpec(memory_space=pl.ANY)] * 6,
        out_specs=vm,
        scratch_shapes=[
            pltpu.VMEM(expert_gate.shape, BF16),
            pltpu.VMEM(expert_up.shape, BF16),
            pltpu.VMEM(expert_down.shape, BF16),
            pltpu.VMEM(shared_gate.shape, BF16),
            pltpu.VMEM(shared_up.shape, BF16),
            pltpu.VMEM(shared_down.shape, BF16),
            pltpu.VMEM((blocks, rows, width), BF16),
            pltpu.VMEM((blocks,) + info.shape, F32),
            pltpu.VMEM((EXP_DEV, 4 * most, width), BF16),
            pltpu.VMEM((2, n_z, EXP_DEV, 4 * most, half), BF16),
            pltpu.VMEM((2, 2, rows, half), BF16),
            pltpu.VMEM((EXP_DEV, 4 * most, cols), BF16),
            pltpu.VMEM((n_z, 2 * per, piece, cols), BF16),
            pltpu.VMEM((n_z, 2 * per, piece, cols), BF16),
            pltpu.VMEM((n_z, 2 * per, piece, cols), BF16),
            pltpu.VMEM((n_z + 1, 2 * per, piece, cols), BF16),
            pltpu.VMEM((2 * per, piece, cols), F32),
            dma((4, blocks, 2)),
            dma((blocks, 2)),
            dma((n_z,)),
            dma((n_z,)),
            dma((2,)),
            dma((n_z,)),
            dma((n_z,)),
            dma((n_z, 2 * per)),
            dma((n_z + 1, 2 * per)),
            dma((6,)),
        ],
        compiler_params=pltpu.CompilerParams(
            collective_id=0, has_side_effects=True, vmem_limit_bytes=64 * 1024 * 1024 - 65536
        ),
    )(
        stream,
        info,
        gain[None, :],
        expert_gate,
        expert_up,
        expert_down,
        shared_gate,
        shared_up,
        shared_down,
    )
    return out.reshape(tokens, cols)


def fits(mesh):
    return mesh.shape["tp"] == 2 and mesh.shape["sp"] in (4, 6, 8)


def solution(mesh):
    return jax.shard_map(
        fast if fits(mesh) else body,
        mesh=mesh,
        in_specs=(
            P(("grp", "sp"), "tp"),
            P(("grp", "sp"), "tp"),
            P(("grp", "sp"), "tp"),
            P(("grp", "sp")),
            P(("grp", "sp"), "tp"),
            P(None, "tp"),
            P("tp"),
            P("tp", None),
            P("tp"),
            P(("grp", "sp"), None),
            P(("grp", "sp"), None),
            P("sp", None, "tp"),
            P("sp", None, "tp"),
            P("sp", None, "tp"),
            P(None, "tp"),
            P(None, "tp"),
            P(None, "tp"),
        ),
        out_specs=P(("grp", "sp"), "tp"),
        check_vma=False,
    )
```

```python
import functools

import jax
import jax.numpy as jnp
from jax import lax
from jax.experimental import pallas as pl
from jax.experimental.pallas import tpu as pltpu
from jax.sharding import PartitionSpec as P

D_CONV = 1024
CONV_K = 3
TOPK = 2
EXP_DEV = 2


def from_behind(value, axis, steps):
    count = lax.axis_size(axis)
    first, last = (max(0, -steps), min(count, count - steps))
    return lax.ppermute(value, axis, [(source, source + steps) for source in range(first, last)])


def body(
    out_gate,
    in_gate,
    conv_input,
    doc_ids,
    residual,
    conv_taps,
    mix_gain,
    out_weight,
    ffn_gain,
    routing,
    route_weight,
    expert_gate,
    expert_up,
    expert_down,
    shared_gate,
    shared_up,
    shared_down,
):
    tokens = residual.shape[0]
    width = out_weight.shape[1]
    n_tp = lax.axis_size("tp")
    n_sp = lax.axis_size("sp")
    rows = tokens // n_tp
    experts = n_sp * EXP_DEV
    most = max(1, 2 * rows * TOPK // experts)
    slots = n_tp * most
    total = experts * slots
    cols = expert_down.shape[2]
    product = (in_gate.astype(jnp.float32) * conv_input.astype(jnp.float32)).astype(jnp.bfloat16)
    tail = (product[tokens - CONV_K + 1 :], doc_ids[tokens - CONV_K + 1 :].astype(jnp.bfloat16))
    prev_rows, prev_docs = from_behind((tail[0], tail[1]), "sp", 1)
    extended = jnp.concatenate([prev_rows, product], axis=0).astype(jnp.float32)
    ext_docs = jnp.concatenate([prev_docs.astype(jnp.int32), doc_ids])
    mixed = jnp.zeros(product.shape, jnp.float32)
    for k in range(CONV_K):
        keep = (ext_docs[k : k + tokens] == doc_ids)[:, None]
        mixed = mixed + jnp.where(keep, conv_taps[k] * extended[k : k + tokens], jnp.float32(0.0))
    conv_out = out_gate.astype(jnp.float32) * mixed
    squares = lax.psum(jnp.sum(conv_out * conv_out, axis=1), "tp")
    normed = (conv_out * lax.rsqrt(squares / D_CONV + 1e-06)[:, None] * mix_gain).astype(
        jnp.bfloat16
    )
    partial_value = jnp.dot(normed, out_weight, preferred_element_type=jnp.float32)
    proj = lax.psum_scatter(
        partial_value.astype(jnp.bfloat16), "tp", scatter_dimension=1, tiled=True
    ).astype(jnp.float32)
    stream = (residual.astype(jnp.float32) + proj).astype(jnp.bfloat16)
    stream32 = stream.astype(jnp.float32)
    stream_sq = lax.psum(jnp.sum(stream32 * stream32, axis=1), "tp")
    normal_cols = (stream32 * lax.rsqrt(stream_sq / width + 1e-06)[:, None] * ffn_gain).astype(
        jnp.bfloat16
    )
    flat_expert = routing.reshape(-1)
    onehot = (flat_expert[:, None] == jnp.arange(experts, dtype=jnp.int32)[None, :]).astype(
        jnp.int32
    )
    blocked = onehot.reshape(n_tp, rows * TOPK, experts)
    earlier = jnp.cumsum(blocked, axis=1) - blocked
    position = jnp.sum(earlier * blocked, axis=2).reshape(-1)
    entry = jnp.arange(tokens * TOPK, dtype=jnp.int32)
    slot = flat_expert * slots + entry // (rows * TOPK) * most + position
    table = jnp.full((total,), tokens, jnp.int32).at[slot].set(entry // TOPK)
    block_rows = lax.all_to_all(normal_cols, "tp", split_axis=0, concat_axis=1, tiled=True)
    mine = lax.dynamic_index_in_dim(
        table.reshape(n_sp, EXP_DEV, n_tp, most), lax.axis_index("tp"), 2, False
    )
    local = jnp.where(mine >= tokens, rows, mine - lax.axis_index("tp") * rows)
    padded_block = jnp.concatenate([block_rows, jnp.zeros((1, width), jnp.bfloat16)], axis=0)
    got = lax.all_to_all(padded_block[local], "sp", split_axis=0, concat_axis=0, tiled=True)
    arrived, whole = (
        lax.all_gather(got, "tp", axis=2, tiled=True),
        lax.all_gather(block_rows.reshape(1, 1, rows, width), "tp", axis=2, tiled=True),
    )
    normal = whole.reshape(tokens, width)
    gate = jnp.einsum("nesd,edh->nesh", arrived, expert_gate, preferred_element_type=jnp.float32)
    upper = jnp.einsum("nesd,edh->nesh", arrived, expert_up, preferred_element_type=jnp.float32)
    hidden = (jax.nn.silu(gate) * upper).astype(jnp.bfloat16)
    hidden_flat = hidden.reshape(n_sp * EXP_DEV * slots, hidden.shape[3])
    shared_hid = (
        jax.nn.silu(jnp.dot(normal, shared_gate, preferred_element_type=jnp.float32))
        * jnp.dot(normal, shared_up, preferred_element_type=jnp.float32)
    ).astype(jnp.bfloat16)
    expert_piece = lax.all_gather(hidden_flat, "tp", axis=1, tiled=True)
    shared_piece = lax.all_gather(shared_hid, "tp", axis=1, tiled=True)
    count = expert_piece.shape[1]
    expert_part = jnp.einsum(
        "nesh,ehd->nesd",
        expert_piece.reshape(n_sp, EXP_DEV, slots, count),
        expert_down,
        preferred_element_type=jnp.float32,
    )
    shared_part = jnp.dot(shared_piece, shared_down, preferred_element_type=jnp.float32)
    returned = lax.all_to_all(
        expert_part.astype(jnp.bfloat16), "sp", split_axis=0, concat_axis=0, tiled=True
    )
    picked = (
        returned.reshape(total, cols)[slot].astype(jnp.float32) * route_weight.reshape(-1)[:, None]
    )
    routed = jnp.sum(picked.reshape(tokens, TOPK, cols), axis=1)
    return (stream32 + shared_part + routed).astype(jnp.bfloat16)


MESH = pl.DeviceIdType.MESH
F32 = jnp.float32
BF16 = jnp.bfloat16


def silu_mul(gate, upper):
    return (gate / (1.0 + jnp.exp(-gate)) * upper).astype(BF16)


def mm(a, b):
    return jnp.dot(a, b, preferred_element_type=F32)


def moe_kernel(
    n_z,
    most,
    own_ref,
    own_meta,
    gain_ref,
    wg_hbm,
    wu_hbm,
    wd_hbm,
    sg_hbm,
    su_hbm,
    sd_hbm,
    out_ref,
    wg,
    wu,
    wd,
    sg,
    su,
    sd,
    blk,
    meta,
    xs,
    hid,
    shid,
    ys,
    acc,
    outgo,
    sib,
    back,
    fin,
    send_sem,
    recv_sem,
    hid_send,
    hid_recv,
    sh_sem,
    sib_send,
    sib_recv,
    back_send,
    back_recv,
    load_sem,
):
    loads = [
        pltpu.make_async_copy(src, dst, load_sem.at[n])
        for n, (src, dst) in enumerate(
            (
                (wg_hbm, wg),
                (wu_hbm, wu),
                (sg_hbm, sg),
                (su_hbm, su),
                (wd_hbm, wd),
                (sd_hbm, sd),
            )
        )
    ]
    for load in loads:
        load.start()
    s = lax.axis_index("sp")
    t = lax.axis_index("tp")
    z = s // 2
    c = s % 2
    rows, width = own_ref.shape
    cols = out_ref.shape[2]
    half = wg.shape[2]
    per, piece = acc.shape[1] // 2, acc.shape[2]
    lo = z > 0
    hi = z < n_z - 1
    up, down = {"sp": s + 2}, {"sp": s - 2}
    other, peer = {"sp": s + 1 - 2 * c}, {"tp": 1 - t}
    targets = (up, down, peer, other)

    def slot(zq, cq, tq):
        return (zq * 2 + cq) * 2 + tq

    def zone(i):
        return z + (1 - 2 * (i % 2)) * ((i + 1) // 2)

    def valid(i):
        zq = zone(i)
        return (i >= 0) & (i <= 2 * n_z - 2) & (zq >= 0) & (zq < n_z)

    def remote(src, dst, ssem, rsem, dev):
        return pltpu.make_async_remote_copy(
            src_ref=src,
            dst_ref=dst,
            send_sem=ssem,
            recv_sem=rsem,
            device_id=dev,
            device_id_type=MESH,
        )

    def block(b, way, own=False):
        return (
            remote(
                own_ref if own else blk.at[b],
                blk.at[b],
                send_sem.at[way, b, 0],
                recv_sem.at[b, 0],
                targets[way],
            ),
            remote(
                own_meta if own else meta.at[b],
                meta.at[b],
                send_sem.at[way, b, 1],
                recv_sem.at[b, 1],
                targets[way],
            ),
        )

    def start(b, way, own=False):
        for copy in block(b, way, own):
            copy.start()

    def arrived(b):
        for copy in block(b, 2):
            copy.wait_recv()

    def hid_copy(zq):
        return remote(hid.at[t, zq], hid.at[t, zq], hid_send.at[zq], hid_recv.at[zq], peer)

    def sh_copy():
        return remote(shid.at[t], shid.at[t], sh_sem.at[0], sh_sem.at[1], peer)

    def sib_copy(zq):
        return remote(outgo.at[zq], sib.at[zq], sib_send.at[zq], sib_recv.at[zq], other)

    def back_copy(zq, q, to, dev):
        return remote(
            acc.at[zq, q],
            back.at[to, q],
            back_send.at[zq, q],
            back_recv.at[to, q],
            dev,
        )

    def pass_on(zq, q):
        @pl.when(zq > z)
        def _():
            back_copy(zq, q, zq, up).start()

        @pl.when(zq < z - 1)
        def _():
            back_copy(zq, q, zq, down).start()

        @pl.when(zq == z - 1)
        def _():
            back_copy(zq, q, n_z, down).start()

    barrier = pltpu.get_barrier_semaphore()
    for way, there in ((0, hi), (1, lo)):

        @pl.when(there)
        def _():
            pl.semaphore_signal(barrier, inc=1, device_id=targets[way], device_id_type=MESH)

    for way in (2, 3):
        pl.semaphore_signal(barrier, inc=1, device_id=targets[way], device_id_type=MESH)
    pl.semaphore_wait(barrier, 2 + lo.astype(jnp.int32) + hi.astype(jnp.int32))

    mine = slot(z, c, t)

    @pl.when(hi)
    def _():
        start(mine, 0, True)

    @pl.when(lo)
    def _():
        start(mine, 1, True)

    start(mine, 2, True)
    start(mine, 3, True)
    blk[mine] = own_ref[...]
    meta[mine] = own_meta[...]

    def picks(b):
        pair = meta[b, z][:, :rows]
        info = jnp.where(c == 0, pair[: 2 * EXP_DEV], pair[2 * EXP_DEV :])
        place = lax.broadcasted_iota(jnp.int32, (most, rows), 0).astype(F32)
        return info, [(info[e : e + 1] == place).astype(F32) for e in range(EXP_DEV)]

    def normalise(value):
        ms = jnp.mean(value * value, axis=1, keepdims=True)
        return (value * lax.rsqrt(ms + 1e-06) * gain_ref[...]).astype(BF16)

    def group(j):
        return [(p, tq, c + p - 2 * c * p) for p in range(2) for tq in range(2)]

    def hidden(zq):
        for j, (p, tq, cq) in enumerate(group(zq)):
            b = slot(zq, cq, tq)
            _, chosen = picks(b)
            sel = jnp.concatenate(chosen, axis=0).astype(BF16)
            got = normalise(mm(sel, blk[b]))
            for e in range(EXP_DEV):
                xs[e, j * most : (j + 1) * most, :] = got[e * most : (e + 1) * most]
        for e in range(EXP_DEV):
            hid[t, zq, e] = silu_mul(mm(xs[e], wg[e]), mm(xs[e], wu[e]))

    def shared():
        for tq in range(2):
            whole = normalise(blk[slot(z, c, tq)].astype(F32))
            shid[t, tq] = silu_mul(mm(whole, sg[...]), mm(whole, su[...]))

    def results(zq):
        hid_copy(zq).wait_recv()
        for e in range(EXP_DEV):
            ys[e] = (
                mm(hid[0, zq, e], wd[e, :half, :]) + mm(hid[1, zq, e], wd[e, half:, :])
            ).astype(BF16)
        for j, (p, tq, cq) in enumerate(group(zq)):
            info, chosen = picks(slot(zq, cq, tq))
            parts = []
            for e in range(EXP_DEV):
                weight = jnp.sum(
                    chosen[e] * info[EXP_DEV + e : EXP_DEV + e + 1], axis=1, keepdims=True
                )
                part = ys[e, j * most : (j + 1) * most, :].astype(F32)
                parts.append((part * weight).astype(BF16))
            sel = jnp.concatenate(chosen, axis=0).astype(BF16)
            spread = lax.dot_general(
                sel,
                jnp.concatenate(parts, axis=0),
                (((0,), (0,)), ((), ())),
                preferred_element_type=F32,
            ).astype(BF16)
            into = acc if p == 0 else outgo
            for h in range(per):
                into[zq, tq * per + h] = spread[h * piece : (h + 1) * piece]
        sib_copy(zq).start()

    def is_end(zq):
        return ((zq > z) & jnp.logical_not(lo)) | ((zq < z) & jnp.logical_not(hi))

    for load in loads[:2]:
        load.wait()

    @pl.loop(1, 2 * n_z + 3)
    def _(i):
        @pl.when(valid(i))
        def _():
            zq = zone(i)
            b = slot(zq, c, t)
            arrived(b)

            @pl.when(hi & (zq < z))
            def _():
                start(b, 0)

            @pl.when(lo & (zq > z))
            def _():
                start(b, 1)

            start(b, 2)
            start(b, 3)

        @pl.when(valid(i - 2))
        def _():
            zq = zone(i - 2)
            b = slot(zq, c, 1 - t)
            arrived(b)
            start(b, 3)
            arrived(slot(zq, 1 - c, t))
            arrived(slot(zq, 1 - c, 1 - t))
            hidden(zq)
            hid_copy(zq).start()

        @pl.when(i == 3)
        def _():
            for load in loads[2:]:
                load.wait()
            shared()

        @pl.when(i == 2 * n_z)
        def _():
            sh_copy().start()

        @pl.when(valid(i - 4))
        def _():
            zq = zone(i - 4)
            results(zq)

            @pl.when(is_end(zq))
            def _():
                sib_copy(zq).wait_recv()
                for q in range(2 * per):
                    acc[zq, q] = (acc[zq, q].astype(F32) + sib[zq, q].astype(F32)).astype(BF16)
                    pass_on(zq, q)

    above = n_z - 1 - z
    up_first = (above >= z).astype(jnp.int32)

    def through(k):
        in_up = (k < above).astype(jnp.int32)
        in_down = (k < z).astype(jnp.int32)
        rise = in_up * (z + 1 + k) + (1 - in_up) * (z - 1 - (k - above))
        fall = in_down * (z - 1 - k) + (1 - in_down) * (z + 1 + (k - z))
        return up_first * rise + (1 - up_first) * fall

    def relay(k, q):
        zq = through(k)

        @pl.when(jnp.logical_not(is_end(zq)))
        def _():
            if q == 0:
                sib_copy(zq).wait_recv()
            back_copy(zq, q, zq, up).wait_recv()
            acc[zq, q] = (
                acc[zq, q].astype(F32) + sib[zq, q].astype(F32) + back[zq, q].astype(F32)
            ).astype(BF16)
            pass_on(zq, q)

    for q in range(2 * per):
        relay(0, q)
    for q in range(2 * per):
        for k in range(1, n_z - 1):
            relay(k, q)

    sib_copy(z).wait_recv()
    sh_copy().wait_recv()
    for tq in range(2):
        stream = blk[slot(z, c, tq), :, pl.ds(pl.multiple_of(t * cols, cols), cols)]
        base = (
            stream.astype(F32)
            + mm(shid[0, tq], sd[:half, :])
            + mm(shid[1, tq], sd[half:, :])
        )
        for h in range(per):
            q = tq * per + h
            fin[q] = (
                base[h * piece : (h + 1) * piece]
                + acc[z, q].astype(F32)
                + sib[z, q].astype(F32)
            )
    for q in range(2 * per):

        @pl.when(lo)
        def _():
            back_copy(z, q, z, up).wait_recv()
            fin[q] = fin[q] + back[z, q].astype(F32)

        @pl.when(hi)
        def _():
            back_copy(z, q, n_z, up).wait_recv()
            fin[q] = fin[q] + back[n_z, q].astype(F32)

        tq, h = divmod(q, per)
        out_ref[tq, h * piece : (h + 1) * piece, :] = fin[q].astype(BF16)

    @pl.loop(0, n_z)
    def _(zq):
        b = slot(zq, c, t)

        @pl.when(hi & (zq <= z))
        def _():
            for copy in block(b, 0):
                copy.wait_send()

        @pl.when(lo & (zq >= z))
        def _():
            for copy in block(b, 1):
                copy.wait_send()

        for copy in block(b, 2) + block(b, 3) + block(slot(zq, c, 1 - t), 3):
            copy.wait_send()
        hid_copy(zq).wait_send()
        sib_copy(zq).wait_send()

        @pl.when(zq != z)
        def _():
            for q in range(2 * per):
                back_copy(zq, q, zq, up).wait_send()

    sh_copy().wait_send()


def fast(
    out_gate,
    in_gate,
    conv_input,
    doc_ids,
    residual,
    conv_taps,
    mix_gain,
    out_weight,
    ffn_gain,
    routing,
    route_weight,
    expert_gate,
    expert_up,
    expert_down,
    shared_gate,
    shared_up,
    shared_down,
):
    tokens, cols = residual.shape
    width = out_weight.shape[1]
    n_tp, n_sp = lax.axis_size("tp"), lax.axis_size("sp")
    n_z = n_sp // 2
    rows = tokens // n_tp
    experts = n_sp * EXP_DEV
    most = max(1, 2 * rows * TOPK // experts)
    t = lax.axis_index("tp")
    swap = [(0, 1), (1, 0)]

    def cut(value, who):
        return lax.dynamic_slice_in_dim(value, who * rows, rows, 0)

    res_other = lax.ppermute(cut(residual, 1 - t), "tp", swap)
    product = (in_gate.astype(F32) * conv_input.astype(F32)).astype(BF16)
    prev_rows, prev_docs = from_behind(
        (product[tokens - CONV_K + 1 :], doc_ids[tokens - CONV_K + 1 :].astype(BF16)), "sp", 1
    )
    extended = jnp.concatenate([prev_rows, product], axis=0).astype(F32)
    ext_docs = jnp.concatenate([prev_docs.astype(jnp.int32), doc_ids])
    mixed = jnp.zeros(product.shape, F32)
    for k in range(CONV_K):
        keep = (ext_docs[k : k + tokens] == doc_ids)[:, None]
        mixed = mixed + jnp.where(keep, conv_taps[k] * extended[k : k + tokens], F32(0.0))
    conv_out = out_gate.astype(F32) * mixed
    sums = jnp.sum(conv_out * conv_out, axis=1)
    sums_other = lax.ppermute(sums, "tp", swap)
    gain_other = lax.ppermute(ffn_gain, "tp", swap)
    squares = sums + sums_other
    first = t == 0
    gain = jnp.concatenate(
        [jnp.where(first, ffn_gain, gain_other), jnp.where(first, gain_other, ffn_gain)]
    )
    normed = (conv_out * lax.rsqrt(squares / D_CONV + 1e-06)[:, None] * mix_gain).astype(BF16)
    given = mm(cut(normed, 1 - t), out_weight).astype(BF16)
    taken = lax.ppermute(given, "tp", swap)
    kept = lax.optimization_barrier(mm(cut(normed, t), out_weight).astype(BF16))
    res_mine = cut(residual, t)
    res = jnp.concatenate(
        [jnp.where(first, res_mine, res_other), jnp.where(first, res_other, res_mine)], axis=1
    )
    stream = (res.astype(F32) + (kept.astype(F32) + taken.astype(F32))).astype(BF16)

    names = cut(routing, t)
    weights = cut(route_weight, t)
    hot = names[:, :, None] == jnp.arange(experts, dtype=jnp.int32)
    named = jnp.any(hot, axis=1)
    placed = jnp.sum(jnp.where(hot, weights[:, :, None], F32(0.0)), axis=1)
    before = jnp.arange(rows)[:, None] > jnp.arange(rows)[None, :]
    earlier = mm(before.astype(BF16), named.astype(BF16))
    position = jnp.where(named, earlier, F32(-1.0))
    info = jnp.stack([position, placed], axis=0).reshape(2, rows, n_sp, EXP_DEV)
    info = info.transpose(2, 0, 3, 1).reshape(n_z, 4 * EXP_DEV, rows)
    pad = -rows % 128
    info = jnp.pad(info, ((0, 0), (0, 0), (0, pad)), constant_values=-1.0)

    per = 4 if rows % 64 == 0 else 1
    piece = rows // per
    blocks = n_sp * n_tp
    half = expert_gate.shape[2]
    vm = pl.BlockSpec(memory_space=pltpu.VMEM)
    dma = pltpu.SemaphoreType.DMA
    out = pl.pallas_call(
        functools.partial(moe_kernel, n_z, most),
        out_shape=jax.ShapeDtypeStruct((n_tp, rows, cols), BF16),
        in_specs=[vm] * 3 + [pl.BlockSpec(memory_space=pl.ANY)] * 6,
        out_specs=vm,
        scratch_shapes=[
            pltpu.VMEM(expert_gate.shape, BF16),
            pltpu.VMEM(expert_up.shape, BF16),
            pltpu.VMEM(expert_down.shape, BF16),
            pltpu.VMEM(shared_gate.shape, BF16),
            pltpu.VMEM(shared_up.shape, BF16),
            pltpu.VMEM(shared_down.shape, BF16),
            pltpu.VMEM((blocks, rows, width), BF16),
            pltpu.VMEM((blocks,) + info.shape, F32),
            pltpu.VMEM((EXP_DEV, 4 * most, width), BF16),
            pltpu.VMEM((2, n_z, EXP_DEV, 4 * most, half), BF16),
            pltpu.VMEM((2, 2, rows, half), BF16),
            pltpu.VMEM((EXP_DEV, 4 * most, cols), BF16),
            pltpu.VMEM((n_z, 2 * per, piece, cols), BF16),
            pltpu.VMEM((n_z, 2 * per, piece, cols), BF16),
            pltpu.VMEM((n_z, 2 * per, piece, cols), BF16),
            pltpu.VMEM((n_z + 1, 2 * per, piece, cols), BF16),
            pltpu.VMEM((2 * per, piece, cols), F32),
            dma((4, blocks, 2)),
            dma((blocks, 2)),
            dma((n_z,)),
            dma((n_z,)),
            dma((2,)),
            dma((n_z,)),
            dma((n_z,)),
            dma((n_z, 2 * per)),
            dma((n_z + 1, 2 * per)),
            dma((6,)),
        ],
        compiler_params=pltpu.CompilerParams(
            collective_id=0, has_side_effects=True, vmem_limit_bytes=64 * 1024 * 1024 - 65536
        ),
    )(
        stream,
        info,
        gain[None, :],
        expert_gate,
        expert_up,
        expert_down,
        shared_gate,
        shared_up,
        shared_down,
    )
    return out.reshape(tokens, cols)


def fits(mesh):
    return mesh.shape["tp"] == 2 and mesh.shape["sp"] in (4, 6, 8)


def solution(mesh):
    return jax.shard_map(
        fast if fits(mesh) else body,
        mesh=mesh,
        in_specs=(
            P(("grp", "sp"), "tp"),
            P(("grp", "sp"), "tp"),
            P(("grp", "sp"), "tp"),
            P(("grp", "sp")),
            P(("grp", "sp"), "tp"),
            P(None, "tp"),
            P("tp"),
            P("tp", None),
            P("tp"),
            P(("grp", "sp"), None),
            P(("grp", "sp"), None),
            P("sp", None, "tp"),
            P("sp", None, "tp"),
            P("sp", None, "tp"),
            P(None, "tp"),
            P(None, "tp"),
            P(None, "tp"),
        ),
        out_specs=P(("grp", "sp"), "tp"),
        check_vma=False,
    )
```

```python
import functools

import jax
import jax.numpy as jnp
from jax import lax
from jax.experimental import pallas as pl
from jax.experimental.pallas import tpu as pltpu
from jax.sharding import PartitionSpec as P

D_CONV = 1024
CONV_K = 3
TOPK = 2
EXP_DEV = 2


def from_behind(value, axis, steps):
    count = lax.axis_size(axis)
    first, last = (max(0, -steps), min(count, count - steps))
    return lax.ppermute(value, axis, [(source, source + steps) for source in range(first, last)])


def body(
    out_gate,
    in_gate,
    conv_input,
    doc_ids,
    residual,
    conv_taps,
    mix_gain,
    out_weight,
    ffn_gain,
    routing,
    route_weight,
    expert_gate,
    expert_up,
    expert_down,
    shared_gate,
    shared_up,
    shared_down,
):
    tokens = residual.shape[0]
    width = out_weight.shape[1]
    n_tp = lax.axis_size("tp")
    n_sp = lax.axis_size("sp")
    rows = tokens // n_tp
    experts = n_sp * EXP_DEV
    most = max(1, 2 * rows * TOPK // experts)
    slots = n_tp * most
    total = experts * slots
    cols = expert_down.shape[2]
    product = (in_gate.astype(jnp.float32) * conv_input.astype(jnp.float32)).astype(jnp.bfloat16)
    tail = (product[tokens - CONV_K + 1 :], doc_ids[tokens - CONV_K + 1 :].astype(jnp.bfloat16))
    prev_rows, prev_docs = from_behind((tail[0], tail[1]), "sp", 1)
    extended = jnp.concatenate([prev_rows, product], axis=0).astype(jnp.float32)
    ext_docs = jnp.concatenate([prev_docs.astype(jnp.int32), doc_ids])
    mixed = jnp.zeros(product.shape, jnp.float32)
    for k in range(CONV_K):
        keep = (ext_docs[k : k + tokens] == doc_ids)[:, None]
        mixed = mixed + jnp.where(keep, conv_taps[k] * extended[k : k + tokens], jnp.float32(0.0))
    conv_out = out_gate.astype(jnp.float32) * mixed
    squares = lax.psum(jnp.sum(conv_out * conv_out, axis=1), "tp")
    normed = (conv_out * lax.rsqrt(squares / D_CONV + 1e-06)[:, None] * mix_gain).astype(
        jnp.bfloat16
    )
    partial_value = jnp.dot(normed, out_weight, preferred_element_type=jnp.float32)
    proj = lax.psum_scatter(
        partial_value.astype(jnp.bfloat16), "tp", scatter_dimension=1, tiled=True
    ).astype(jnp.float32)
    stream = (residual.astype(jnp.float32) + proj).astype(jnp.bfloat16)
    stream32 = stream.astype(jnp.float32)
    stream_sq = lax.psum(jnp.sum(stream32 * stream32, axis=1), "tp")
    normal_cols = (stream32 * lax.rsqrt(stream_sq / width + 1e-06)[:, None] * ffn_gain).astype(
        jnp.bfloat16
    )
    flat_expert = routing.reshape(-1)
    onehot = (flat_expert[:, None] == jnp.arange(experts, dtype=jnp.int32)[None, :]).astype(
        jnp.int32
    )
    blocked = onehot.reshape(n_tp, rows * TOPK, experts)
    earlier = jnp.cumsum(blocked, axis=1) - blocked
    position = jnp.sum(earlier * blocked, axis=2).reshape(-1)
    entry = jnp.arange(tokens * TOPK, dtype=jnp.int32)
    slot = flat_expert * slots + entry // (rows * TOPK) * most + position
    table = jnp.full((total,), tokens, jnp.int32).at[slot].set(entry // TOPK)
    block_rows = lax.all_to_all(normal_cols, "tp", split_axis=0, concat_axis=1, tiled=True)
    mine = lax.dynamic_index_in_dim(
        table.reshape(n_sp, EXP_DEV, n_tp, most), lax.axis_index("tp"), 2, False
    )
    local = jnp.where(mine >= tokens, rows, mine - lax.axis_index("tp") * rows)
    padded_block = jnp.concatenate([block_rows, jnp.zeros((1, width), jnp.bfloat16)], axis=0)
    got = lax.all_to_all(padded_block[local], "sp", split_axis=0, concat_axis=0, tiled=True)
    arrived, whole = (
        lax.all_gather(got, "tp", axis=2, tiled=True),
        lax.all_gather(block_rows.reshape(1, 1, rows, width), "tp", axis=2, tiled=True),
    )
    normal = whole.reshape(tokens, width)
    gate = jnp.einsum("nesd,edh->nesh", arrived, expert_gate, preferred_element_type=jnp.float32)
    upper = jnp.einsum("nesd,edh->nesh", arrived, expert_up, preferred_element_type=jnp.float32)
    hidden = (jax.nn.silu(gate) * upper).astype(jnp.bfloat16)
    hidden_flat = hidden.reshape(n_sp * EXP_DEV * slots, hidden.shape[3])
    shared_hid = (
        jax.nn.silu(jnp.dot(normal, shared_gate, preferred_element_type=jnp.float32))
        * jnp.dot(normal, shared_up, preferred_element_type=jnp.float32)
    ).astype(jnp.bfloat16)
    expert_piece = lax.all_gather(hidden_flat, "tp", axis=1, tiled=True)
    shared_piece = lax.all_gather(shared_hid, "tp", axis=1, tiled=True)
    count = expert_piece.shape[1]
    expert_part = jnp.einsum(
        "nesh,ehd->nesd",
        expert_piece.reshape(n_sp, EXP_DEV, slots, count),
        expert_down,
        preferred_element_type=jnp.float32,
    )
    shared_part = jnp.dot(shared_piece, shared_down, preferred_element_type=jnp.float32)
    returned = lax.all_to_all(
        expert_part.astype(jnp.bfloat16), "sp", split_axis=0, concat_axis=0, tiled=True
    )
    picked = (
        returned.reshape(total, cols)[slot].astype(jnp.float32) * route_weight.reshape(-1)[:, None]
    )
    routed = jnp.sum(picked.reshape(tokens, TOPK, cols), axis=1)
    return (stream32 + shared_part + routed).astype(jnp.bfloat16)


MESH = pl.DeviceIdType.MESH
F32 = jnp.float32
BF16 = jnp.bfloat16


def silu_mul(gate, upper):
    return (gate / (1.0 + jnp.exp(-gate)) * upper).astype(BF16)


def mm(a, b):
    return jnp.dot(a, b, preferred_element_type=F32)


def moe_kernel(
    n_z,
    most,
    own_ref,
    own_meta,
    gain_ref,
    wg_hbm,
    wu_hbm,
    wd_hbm,
    sg_hbm,
    su_hbm,
    sd_hbm,
    out_ref,
    wg,
    wu,
    wd,
    sg,
    su,
    sd,
    blk,
    meta,
    xs,
    hid,
    shid,
    ys,
    acc,
    outgo,
    sib,
    back,
    fin,
    send_sem,
    recv_sem,
    hid_send,
    hid_recv,
    sh_sem,
    sib_send,
    sib_recv,
    back_send,
    back_recv,
    load_sem,
):
    loads = [
        pltpu.make_async_copy(src, dst, load_sem.at[n])
        for n, (src, dst) in enumerate(
            (
                (wg_hbm, wg),
                (wu_hbm, wu),
                (sg_hbm, sg),
                (su_hbm, su),
                (wd_hbm, wd),
                (sd_hbm, sd),
            )
        )
    ]
    for load in loads:
        load.start()
    s = lax.axis_index("sp")
    t = lax.axis_index("tp")
    z = s // 2
    c = s % 2
    rows, width = own_ref.shape
    cols = out_ref.shape[2]
    half = wg.shape[2]
    per, piece = acc.shape[1] // 2, acc.shape[2]
    lo = z > 0
    hi = z < n_z - 1
    up, down = {"sp": s + 2}, {"sp": s - 2}
    other, peer = {"sp": s + 1 - 2 * c}, {"tp": 1 - t}
    targets = (up, down, peer, other)

    def slot(zq, cq, tq):
        return (zq * 2 + cq) * 2 + tq

    def zone(i):
        return z + (1 - 2 * (i % 2)) * ((i + 1) // 2)

    def valid(i):
        zq = zone(i)
        return (i >= 0) & (i <= 2 * n_z - 2) & (zq >= 0) & (zq < n_z)

    def remote(src, dst, ssem, rsem, dev):
        return pltpu.make_async_remote_copy(
            src_ref=src,
            dst_ref=dst,
            send_sem=ssem,
            recv_sem=rsem,
            device_id=dev,
            device_id_type=MESH,
        )

    def block(b, way, own=False):
        return (
            remote(
                own_ref if own else blk.at[b],
                blk.at[b],
                send_sem.at[way, b, 0],
                recv_sem.at[b, 0],
                targets[way],
            ),
            remote(
                own_meta if own else meta.at[b],
                meta.at[b],
                send_sem.at[way, b, 1],
                recv_sem.at[b, 1],
                targets[way],
            ),
        )

    def start(b, way, own=False):
        for copy in block(b, way, own):
            copy.start()

    def arrived(b):
        for copy in block(b, 2):
            copy.wait_recv()

    def hid_copy(zq):
        return remote(hid.at[t, zq], hid.at[t, zq], hid_send.at[zq], hid_recv.at[zq], peer)

    def sh_copy():
        return remote(shid.at[t], shid.at[t], sh_sem.at[0], sh_sem.at[1], peer)

    def sib_copy(zq):
        return remote(outgo.at[zq], sib.at[zq], sib_send.at[zq], sib_recv.at[zq], other)

    def back_copy(zq, q, to, dev):
        return remote(
            acc.at[zq, q],
            back.at[to, q],
            back_send.at[zq, q],
            back_recv.at[to, q],
            dev,
        )

    def pass_on(zq, q):
        @pl.when(zq > z)
        def _():
            back_copy(zq, q, zq, up).start()

        @pl.when(zq < z - 1)
        def _():
            back_copy(zq, q, zq, down).start()

        @pl.when(zq == z - 1)
        def _():
            back_copy(zq, q, n_z, down).start()

    barrier = pltpu.get_barrier_semaphore()
    for way, there in ((0, hi), (1, lo)):

        @pl.when(there)
        def _():
            pl.semaphore_signal(barrier, inc=1, device_id=targets[way], device_id_type=MESH)

    for way in (2, 3):
        pl.semaphore_signal(barrier, inc=1, device_id=targets[way], device_id_type=MESH)
    pl.semaphore_wait(barrier, 2 + lo.astype(jnp.int32) + hi.astype(jnp.int32))

    mine = slot(z, c, t)

    @pl.when(hi)
    def _():
        start(mine, 0, True)

    @pl.when(lo)
    def _():
        start(mine, 1, True)

    start(mine, 2, True)
    start(mine, 3, True)
    blk[mine] = own_ref[...]
    meta[mine] = own_meta[...]

    def picks(b):
        pair = meta[b, z][:, :rows]
        info = jnp.where(c == 0, pair[: 2 * EXP_DEV], pair[2 * EXP_DEV :])
        place = lax.broadcasted_iota(jnp.int32, (most, rows), 0).astype(F32)
        return info, [(info[e : e + 1] == place).astype(F32) for e in range(EXP_DEV)]

    def normalise(value):
        ms = jnp.mean(value * value, axis=1, keepdims=True)
        return (value * lax.rsqrt(ms + 1e-06) * gain_ref[...]).astype(BF16)

    def group(j):
        return [(p, tq, c + p - 2 * c * p) for p in range(2) for tq in range(2)]

    def hidden(zq):
        for j, (p, tq, cq) in enumerate(group(zq)):
            b = slot(zq, cq, tq)
            _, chosen = picks(b)
            sel = jnp.concatenate(chosen, axis=0).astype(BF16)
            got = normalise(mm(sel, blk[b]))
            for e in range(EXP_DEV):
                xs[e, j * most : (j + 1) * most, :] = got[e * most : (e + 1) * most]
        for e in range(EXP_DEV):
            hid[t, zq, e] = silu_mul(mm(xs[e], wg[e]), mm(xs[e], wu[e]))

    def shared():
        for tq in range(2):
            whole = normalise(blk[slot(z, c, tq)].astype(F32))
            shid[t, tq] = silu_mul(mm(whole, sg[...]), mm(whole, su[...]))

    def results(zq):
        hid_copy(zq).wait_recv()
        for e in range(EXP_DEV):
            ys[e] = (
                mm(hid[0, zq, e], wd[e, :half, :]) + mm(hid[1, zq, e], wd[e, half:, :])
            ).astype(BF16)
        for j, (p, tq, cq) in enumerate(group(zq)):
            info, chosen = picks(slot(zq, cq, tq))
            parts = []
            for e in range(EXP_DEV):
                weight = jnp.sum(
                    chosen[e] * info[EXP_DEV + e : EXP_DEV + e + 1], axis=1, keepdims=True
                )
                part = ys[e, j * most : (j + 1) * most, :].astype(F32)
                parts.append((part * weight).astype(BF16))
            sel = jnp.concatenate(chosen, axis=0).astype(BF16)
            spread = lax.dot_general(
                sel,
                jnp.concatenate(parts, axis=0),
                (((0,), (0,)), ((), ())),
                preferred_element_type=F32,
            ).astype(BF16)
            into = acc if p == 0 else outgo
            for h in range(per):
                into[zq, tq * per + h] = spread[h * piece : (h + 1) * piece]
        sib_copy(zq).start()

    def is_end(zq):
        return ((zq > z) & jnp.logical_not(lo)) | ((zq < z) & jnp.logical_not(hi))

    for load in loads[:2]:
        load.wait()

    @pl.loop(1, 2 * n_z + 3)
    def _(i):
        @pl.when(valid(i))
        def _():
            zq = zone(i)
            b = slot(zq, c, t)
            arrived(b)

            @pl.when(hi & (zq < z))
            def _():
                start(b, 0)

            @pl.when(lo & (zq > z))
            def _():
                start(b, 1)

            start(b, 2)
            start(b, 3)

        @pl.when(valid(i - 4))
        def _():
            zq = zone(i - 4)
            results(zq)

            @pl.when(is_end(zq))
            def _():
                sib_copy(zq).wait_recv()
                for q in range(2 * per):
                    acc[zq, q] = (acc[zq, q].astype(F32) + sib[zq, q].astype(F32)).astype(BF16)
                    pass_on(zq, q)

        @pl.when(valid(i - 2))
        def _():
            zq = zone(i - 2)
            b = slot(zq, c, 1 - t)
            arrived(b)
            start(b, 3)
            arrived(slot(zq, 1 - c, t))
            arrived(slot(zq, 1 - c, 1 - t))
            hidden(zq)
            hid_copy(zq).start()

        @pl.when(i == 3)
        def _():
            for load in loads[2:]:
                load.wait()
            shared()

        @pl.when(i == 2 * n_z)
        def _():
            sh_copy().start()


    above = n_z - 1 - z
    up_first = (above >= z).astype(jnp.int32)

    def through(k):
        in_up = (k < above).astype(jnp.int32)
        in_down = (k < z).astype(jnp.int32)
        rise = in_up * (z + 1 + k) + (1 - in_up) * (z - 1 - (k - above))
        fall = in_down * (z - 1 - k) + (1 - in_down) * (z + 1 + (k - z))
        return up_first * rise + (1 - up_first) * fall

    def relay(k, q):
        zq = through(k)

        @pl.when(jnp.logical_not(is_end(zq)))
        def _():
            if q == 0:
                sib_copy(zq).wait_recv()
            back_copy(zq, q, zq, up).wait_recv()
            acc[zq, q] = (
                acc[zq, q].astype(F32) + sib[zq, q].astype(F32) + back[zq, q].astype(F32)
            ).astype(BF16)
            pass_on(zq, q)

    for q in range(2 * per):
        relay(0, q)
    for q in range(2 * per):
        for k in range(1, n_z - 1):
            relay(k, q)

    sib_copy(z).wait_recv()
    sh_copy().wait_recv()
    for tq in range(2):
        stream = blk[slot(z, c, tq), :, pl.ds(pl.multiple_of(t * cols, cols), cols)]
        base = (
            stream.astype(F32)
            + mm(shid[0, tq], sd[:half, :])
            + mm(shid[1, tq], sd[half:, :])
        )
        for h in range(per):
            q = tq * per + h
            fin[q] = (
                base[h * piece : (h + 1) * piece]
                + acc[z, q].astype(F32)
                + sib[z, q].astype(F32)
            )
    for q in range(2 * per):

        @pl.when(lo)
        def _():
            back_copy(z, q, z, up).wait_recv()
            fin[q] = fin[q] + back[z, q].astype(F32)

        @pl.when(hi)
        def _():
            back_copy(z, q, n_z, up).wait_recv()
            fin[q] = fin[q] + back[n_z, q].astype(F32)

        tq, h = divmod(q, per)
        out_ref[tq, h * piece : (h + 1) * piece, :] = fin[q].astype(BF16)

    @pl.loop(0, n_z)
    def _(zq):
        b = slot(zq, c, t)

        @pl.when(hi & (zq <= z))
        def _():
            for copy in block(b, 0):
                copy.wait_send()

        @pl.when(lo & (zq >= z))
        def _():
            for copy in block(b, 1):
                copy.wait_send()

        for copy in block(b, 2) + block(b, 3) + block(slot(zq, c, 1 - t), 3):
            copy.wait_send()
        hid_copy(zq).wait_send()
        sib_copy(zq).wait_send()

        @pl.when(zq != z)
        def _():
            for q in range(2 * per):
                back_copy(zq, q, zq, up).wait_send()

    sh_copy().wait_send()


def fast(
    out_gate,
    in_gate,
    conv_input,
    doc_ids,
    residual,
    conv_taps,
    mix_gain,
    out_weight,
    ffn_gain,
    routing,
    route_weight,
    expert_gate,
    expert_up,
    expert_down,
    shared_gate,
    shared_up,
    shared_down,
):
    tokens, cols = residual.shape
    width = out_weight.shape[1]
    n_tp, n_sp = lax.axis_size("tp"), lax.axis_size("sp")
    n_z = n_sp // 2
    rows = tokens // n_tp
    experts = n_sp * EXP_DEV
    most = max(1, 2 * rows * TOPK // experts)
    t = lax.axis_index("tp")
    swap = [(0, 1), (1, 0)]

    def cut(value, who):
        return lax.dynamic_slice_in_dim(value, who * rows, rows, 0)

    res_other = lax.ppermute(cut(residual, 1 - t), "tp", swap)
    product = (in_gate.astype(F32) * conv_input.astype(F32)).astype(BF16)
    prev_rows, prev_docs = from_behind(
        (product[tokens - CONV_K + 1 :], doc_ids[tokens - CONV_K + 1 :].astype(BF16)), "sp", 1
    )
    extended = jnp.concatenate([prev_rows, product], axis=0).astype(F32)
    ext_docs = jnp.concatenate([prev_docs.astype(jnp.int32), doc_ids])
    mixed = jnp.zeros(product.shape, F32)
    for k in range(CONV_K):
        keep = (ext_docs[k : k + tokens] == doc_ids)[:, None]
        mixed = mixed + jnp.where(keep, conv_taps[k] * extended[k : k + tokens], F32(0.0))
    conv_out = out_gate.astype(F32) * mixed
    sums = jnp.sum(conv_out * conv_out, axis=1)
    sums_other = lax.ppermute(sums, "tp", swap)
    gain_other = lax.ppermute(ffn_gain, "tp", swap)
    squares = sums + sums_other
    first = t == 0
    gain = jnp.concatenate(
        [jnp.where(first, ffn_gain, gain_other), jnp.where(first, gain_other, ffn_gain)]
    )
    normed = (conv_out * lax.rsqrt(squares / D_CONV + 1e-06)[:, None] * mix_gain).astype(BF16)
    given = mm(cut(normed, 1 - t), out_weight).astype(BF16)
    taken = lax.ppermute(given, "tp", swap)
    kept = lax.optimization_barrier(mm(cut(normed, t), out_weight).astype(BF16))
    res_mine = cut(residual, t)
    res = jnp.concatenate(
        [jnp.where(first, res_mine, res_other), jnp.where(first, res_other, res_mine)], axis=1
    )
    stream = (res.astype(F32) + (kept.astype(F32) + taken.astype(F32))).astype(BF16)

    names = cut(routing, t)
    weights = cut(route_weight, t)
    hot = names[:, :, None] == jnp.arange(experts, dtype=jnp.int32)
    named = jnp.any(hot, axis=1)
    placed = jnp.sum(jnp.where(hot, weights[:, :, None], F32(0.0)), axis=1)
    before = jnp.arange(rows)[:, None] > jnp.arange(rows)[None, :]
    earlier = mm(before.astype(BF16), named.astype(BF16))
    position = jnp.where(named, earlier, F32(-1.0))
    info = jnp.stack([position, placed], axis=0).reshape(2, rows, n_sp, EXP_DEV)
    info = info.transpose(2, 0, 3, 1).reshape(n_z, 4 * EXP_DEV, rows)
    pad = -rows % 128
    info = jnp.pad(info, ((0, 0), (0, 0), (0, pad)), constant_values=-1.0)

    per = 2
    piece = rows // per
    blocks = n_sp * n_tp
    half = expert_gate.shape[2]
    vm = pl.BlockSpec(memory_space=pltpu.VMEM)
    dma = pltpu.SemaphoreType.DMA
    out = pl.pallas_call(
        functools.partial(moe_kernel, n_z, most),
        out_shape=jax.ShapeDtypeStruct((n_tp, rows, cols), BF16),
        in_specs=[vm] * 3 + [pl.BlockSpec(memory_space=pl.ANY)] * 6,
        out_specs=vm,
        scratch_shapes=[
            pltpu.VMEM(expert_gate.shape, BF16),
            pltpu.VMEM(expert_up.shape, BF16),
            pltpu.VMEM(expert_down.shape, BF16),
            pltpu.VMEM(shared_gate.shape, BF16),
            pltpu.VMEM(shared_up.shape, BF16),
            pltpu.VMEM(shared_down.shape, BF16),
            pltpu.VMEM((blocks, rows, width), BF16),
            pltpu.VMEM((blocks,) + info.shape, F32),
            pltpu.VMEM((EXP_DEV, 4 * most, width), BF16),
            pltpu.VMEM((2, n_z, EXP_DEV, 4 * most, half), BF16),
            pltpu.VMEM((2, 2, rows, half), BF16),
            pltpu.VMEM((EXP_DEV, 4 * most, cols), BF16),
            pltpu.VMEM((n_z, 2 * per, piece, cols), BF16),
            pltpu.VMEM((n_z, 2 * per, piece, cols), BF16),
            pltpu.VMEM((n_z, 2 * per, piece, cols), BF16),
            pltpu.VMEM((n_z + 1, 2 * per, piece, cols), BF16),
            pltpu.VMEM((2 * per, piece, cols), F32),
            dma((4, blocks, 2)),
            dma((blocks, 2)),
            dma((n_z,)),
            dma((n_z,)),
            dma((2,)),
            dma((n_z,)),
            dma((n_z,)),
            dma((n_z, 2 * per)),
            dma((n_z + 1, 2 * per)),
            dma((6,)),
        ],
        compiler_params=pltpu.CompilerParams(
            collective_id=0, has_side_effects=True, vmem_limit_bytes=64 * 1024 * 1024 - 65536
        ),
    )(
        stream,
        info,
        gain[None, :],
        expert_gate,
        expert_up,
        expert_down,
        shared_gate,
        shared_up,
        shared_down,
    )
    return out.reshape(tokens, cols)


def fits(mesh):
    return mesh.shape["tp"] == 2 and mesh.shape["sp"] in (4, 6, 8)


def solution(mesh):
    return jax.shard_map(
        fast if fits(mesh) else body,
        mesh=mesh,
        in_specs=(
            P(("grp", "sp"), "tp"),
            P(("grp", "sp"), "tp"),
            P(("grp", "sp"), "tp"),
            P(("grp", "sp")),
            P(("grp", "sp"), "tp"),
            P(None, "tp"),
            P("tp"),
            P("tp", None),
            P("tp"),
            P(("grp", "sp"), None),
            P(("grp", "sp"), None),
            P("sp", None, "tp"),
            P("sp", None, "tp"),
            P("sp", None, "tp"),
            P(None, "tp"),
            P(None, "tp"),
            P(None, "tp"),
        ),
        out_specs=P(("grp", "sp"), "tp"),
        check_vma=False,
    )
```
